768 devices in a mesh: sp: 96 (over z, y), tp: 8 (over x, core).
Axes of the slice: x: 4, y: 8, z: 12, core: 2. Of those that a mesh axis runs over, the one named last changes fastest.
Arguments:
- latents: bfloat16 [61440, 2048], P('sp'), may hold values from -6 to 6
- cond: float32 [2048], replicated, may hold values from -6 to 6
- ctx_cond: float32 [2048], replicated, may hold values from -6 to 6
- context: bfloat16 [768, 2048], P('sp'), may hold values from -6 to 6
- norm_gain: float32 [2048], replicated, may hold values from 0.1 to 1.9
- shift_weight: bfloat16 [2048, 2048], P('tp'), may hold values from -0.125 to 0.125
- scale_weight: bfloat16 [2048, 2048], P('tp'), may hold values from -0.125 to 0.125
- gate_weight: bfloat16 [2048, 2048], P('tp'), may hold values from -0.125 to 0.125
- q_weight: bfloat16 [2048, 1024], P(None, 'tp'), may hold values from -0.125 to 0.125
- k_weight: bfloat16 [2048, 1024], P(None, 'tp'), may hold values from -0.125 to 0.125
- v_weight: bfloat16 [2048, 1024], P(None, 'tp'), may hold values from -0.125 to 0.125
- out_weight: bfloat16 [1024, 2048], replicated, may hold values from -1.5 to 1.5
- rel_bias: float32 [8, 15, 31], P('tp'), may hold values from 1.5 to 260
Outputs:
- result: bfloat16 [61440, 2048], P(('sp', 'tp'))
The draws below stay inside these ranges and needn't reach their ends.
All inputs are finite; a program needn't handle non-finite values.
Results may differ from the reference program's by a relative error of at most 0.0085.
Values may be sent and summed in bfloat16 or wider, within the bound.
A program may use at most 64 MiB of HBM per device.

```python
import jax
import jax.numpy as jnp
from jax import lax

D = 2048
HEADS = 8
HEAD_DIM = 128
GRID_W = 64
WIN_ROWS = 8
WIN_COLS = 16
CTX = 768
ROWS = 960
TOKENS = 61440
NA_WIDTH = 1024


def draw_rel_bias(key, part):
    base_key = jax.random.fold_in(jax.random.fold_in(key, 4711), 0)
    table = jax.random.uniform(base_key, (HEADS, 2 * WIN_ROWS - 1, 2 * WIN_COLS - 1), jnp.float32, 1.5, 4.5)
    return table.astype(jnp.float32)


def block_scale(own_key, extent, cuts, low, top_value):
    def one(axis_at, parts):
        steps = jax.random.uniform(jax.random.fold_in(jax.random.fold_in(own_key, 6), axis_at), (parts,), jnp.float32, low / len(cuts), top_value / len(cuts))
        return jnp.repeat(jnp.exp(steps), extent[axis_at] // parts).reshape((-1,) + (1,) * (len(extent) - axis_at - 1))

    level = one(*cuts[0])
    for cut in cuts[1:]:
        level = level * one(*cut)
    return level


def noise(stream_key, shape, width, limit, cuts=(), kind=jnp.bfloat16):
    level = block_scale(stream_key, shape, cuts, -0.22, 0.18) if cuts else 1.0
    array = jax.random.normal(stream_key, shape, jnp.float32) * width * level
    return jnp.minimum(jnp.maximum(array, -limit), limit).astype(kind)


def setup_inputs(seed: int = 0) -> dict:
    key_list = jax.random.split(jax.random.key(seed), 14)
    return {
        "latents": noise(key_list[0], (TOKENS, D), 1.0, 6.0, ((0, 96),)),
        "cond": noise(key_list[1], (D,), 1.0, 6.0, (), jnp.float32),
        "ctx_cond": noise(key_list[2], (D,), 1.0, 6.0, (), jnp.float32),
        "context": noise(key_list[3], (CTX, D), 1.0, 6.0, ((0, 96),)),
        "norm_gain": jnp.clip(1.0 + 0.18 * jax.random.normal(key_list[4], (D,), jnp.float32), 0.1, 1.9),
        "shift_weight": noise(key_list[5], (D, D), D ** -0.5, 0.125, ((0, 8),)),
        "scale_weight": noise(key_list[6], (D, D), D ** -0.5, 0.125, ((0, 8),)),
        "gate_weight": noise(key_list[7], (D, D), D ** -0.5, 0.125, ((0, 8),)),
        "q_weight": noise(key_list[8], (D, NA_WIDTH), D ** -0.5, 0.125, ((1, 8),)),
        "k_weight": noise(key_list[9], (D, NA_WIDTH), D ** -0.5, 0.125, ((1, 8),)),
        "v_weight": noise(key_list[10], (D, NA_WIDTH), D ** -0.5, 0.125, ((1, 8),)),
        "out_weight": noise(key_list[11], (NA_WIDTH, D), (max(NA_WIDTH // 64, 1)) ** -0.5, 1.5),
        "rel_bias": draw_rel_bias(jax.random.fold_in(key_list[13], 71), 0),
    }


EPS = 1e-06
NEG_BIG = -1e+30

def modulated_norm(tok_rows, gain, shift_row, scale_row):
    rows_f = tok_rows.astype(jnp.float32)
    inverse = lax.rsqrt(lax.optimization_barrier(jnp.mean(rows_f * rows_f, axis=-1, keepdims=True)) + EPS)
    return (rows_f * inverse * gain * (1.0 + scale_row) + shift_row).astype(jnp.bfloat16)

def column_mask():
    columns = jnp.arange(GRID_W, dtype=jnp.int32)
    first_col = jnp.clip(columns - WIN_COLS // 2, 0, GRID_W - WIN_COLS)
    inside = (columns[None, :] >= first_col[:, None]) & (columns[None, :] < first_col[:, None] + WIN_COLS)
    return jnp.tile(inside, (1, WIN_ROWS))

def grid_bias(bias_table, row_diff):
    row_hot = (row_diff[:, :, None] == jnp.arange(2 * WIN_ROWS - 1, dtype=jnp.int32)[None, None, :]).astype(jnp.float32)
    columns = jnp.arange(GRID_W, dtype=jnp.int32)
    col_diff = jnp.clip(columns[None, :] - columns[:, None], -(WIN_COLS - 1), WIN_COLS - 1) + WIN_COLS - 1
    col_hot = (col_diff[:, :, None] == jnp.arange(2 * WIN_COLS - 1, dtype=jnp.int32)[None, None, :]).astype(jnp.float32)
    middle = jnp.einsum('rai,hij->hraj', row_hot, bias_table.astype(jnp.float32), precision=lax.Precision.HIGHEST)
    spread = jnp.einsum('hraj,qbj->hrqab', middle, col_hot, precision=lax.Precision.HIGHEST)
    return spread.reshape(bias_table.shape[0], row_diff.shape[0], GRID_W, WIN_ROWS * GRID_W)

def attend(query, key_win, val_win, ctx_keys, ctx_vals, bias, inside):
    factor = HEAD_DIM ** (-0.5)
    near_scores = jnp.einsum('rqhd,rkhd->hrqk', query.astype(jnp.float32), key_win.astype(jnp.float32)) * factor + bias
    near_scores = jnp.where(inside, near_scores, NEG_BIG)
    far_scores = jnp.einsum('rqhd,lhd->hrql', query.astype(jnp.float32), ctx_keys.astype(jnp.float32)) * factor
    row_peak = jnp.maximum(lax.optimization_barrier(jnp.max(near_scores, axis=-1, keepdims=True)), lax.optimization_barrier(jnp.max(far_scores, axis=-1, keepdims=True)))
    near_exp = jnp.exp(near_scores - row_peak)
    far_exp = jnp.exp(far_scores - row_peak)
    denominator = lax.optimization_barrier(jnp.sum(near_exp, axis=-1, keepdims=True)) + lax.optimization_barrier(jnp.sum(far_exp, axis=-1, keepdims=True))
    near_w = (near_exp / denominator).astype(jnp.bfloat16)
    far_w = (far_exp / denominator).astype(jnp.bfloat16)
    mixed = jnp.einsum('hrqk,rkhd->rqhd', near_w.astype(jnp.float32), val_win.astype(jnp.float32)) + jnp.einsum('hrql,lhd->rqhd', far_w.astype(jnp.float32), ctx_vals.astype(jnp.float32))
    return mixed.astype(jnp.bfloat16)

def reference(latents, cond, ctx_cond, context, norm_gain, shift_weight, scale_weight, gate_weight, q_weight, k_weight, v_weight, out_weight, rel_bias):
    conds = jnp.stack([cond, ctx_cond])
    active = jax.nn.silu(conds).astype(jnp.bfloat16)
    shifts = jnp.dot(active, shift_weight, preferred_element_type=jnp.float32)
    scales = jnp.dot(active, scale_weight, preferred_element_type=jnp.float32)
    gates = jnp.dot(active[:1], gate_weight, preferred_element_type=jnp.float32)
    h_lat = modulated_norm(latents, norm_gain, shifts[0], scales[0])
    h_ctx = modulated_norm(context, norm_gain, shifts[1], scales[1])
    query = jnp.dot(h_lat, q_weight, preferred_element_type=jnp.float32).astype(jnp.bfloat16)
    keys = jnp.dot(h_lat, k_weight, preferred_element_type=jnp.float32).astype(jnp.bfloat16)
    values = jnp.dot(h_lat, v_weight, preferred_element_type=jnp.float32).astype(jnp.bfloat16)
    ctx_keys = jnp.dot(h_ctx, k_weight, preferred_element_type=jnp.float32).astype(jnp.bfloat16)
    ctx_vals = jnp.dot(h_ctx, v_weight, preferred_element_type=jnp.float32).astype(jnp.bfloat16)
    grid_rows = jnp.arange(ROWS, dtype=jnp.int32)
    first_row = jnp.clip(grid_rows - WIN_ROWS // 2, 0, ROWS - WIN_ROWS)
    offsets = jnp.arange(WIN_ROWS, dtype=jnp.int32)
    row_index = first_row[:, None] + offsets[None, :]
    row_diff = row_index - grid_rows[:, None] + WIN_ROWS - 1
    inside = column_mask()
    query_grid = query.reshape(ROWS, GRID_W, HEADS, HEAD_DIM)
    key_grid = keys.reshape(ROWS, GRID_W, HEADS, HEAD_DIM)
    val_grid = values.reshape(ROWS, GRID_W, HEADS, HEAD_DIM)
    ctx_key3 = ctx_keys.reshape(CTX, HEADS, HEAD_DIM)
    ctx_val3 = ctx_vals.reshape(CTX, HEADS, HEAD_DIM)

    def one_head(head_id):
        query_head = lax.dynamic_slice_in_dim(query_grid, head_id, 1, 2)
        key_head = lax.dynamic_slice_in_dim(key_grid, head_id, 1, 2)[row_index]
        val_head = lax.dynamic_slice_in_dim(val_grid, head_id, 1, 2)[row_index]
        key_head = key_head.reshape(ROWS, WIN_ROWS * GRID_W, 1, HEAD_DIM)
        val_head = val_head.reshape(ROWS, WIN_ROWS * GRID_W, 1, HEAD_DIM)
        ctx_key_head = lax.dynamic_slice_in_dim(ctx_key3, head_id, 1, 1)
        ctx_val_head = lax.dynamic_slice_in_dim(ctx_val3, head_id, 1, 1)
        bias = grid_bias(lax.dynamic_slice_in_dim(rel_bias, head_id, 1, 0), row_diff)
        return attend(query_head, key_head, val_head, ctx_key_head, ctx_val_head, bias, inside)
    head_outs = lax.map(one_head, jnp.arange(HEADS, dtype=jnp.int32))
    attn = jnp.transpose(head_outs[:, :, :, 0], (1, 2, 0, 3)).reshape(TOKENS, NA_WIDTH)
    mixed = jnp.dot(attn, out_weight, preferred_element_type=jnp.float32)
    return (latents.astype(jnp.float32) + gates[0] * mixed).astype(jnp.bfloat16)
```

```python
import jax
import jax.numpy as jnp
from jax import lax
from jax.experimental import pallas as pl
from jax.experimental.pallas import tpu as pltpu
from jax.sharding import PartitionSpec as P

D = 2048
HD = 128
GW = 64
WR = 8
WC = 16
EPS = 1e-06
NEG = -1e30
ZN, YN, XN = 12, 8, 4
NT = D // 128
TOK = 640
ROWS = TOK // GW
ALL_ROWS = ROWS * ZN * YN
BEFORE, AFTER = 4, 3
OWN = BEFORE * GW
KVN = (BEFORE + ROWS + AFTER) * GW
CR = 8
CB = CR * ZN
F32 = jnp.float32
BF16 = jnp.bfloat16
NT_DIMS = (((1,), (1,)), ((), ()))


def body(
    lat_h, cond_h, cctx_h, ctx_h, gain_h, shw_h, scw_h, gtw_h, qw_h, kw_h, vw_h, ow_h, rb_h,
    out_ref,
    lat, cond, cctx, craw, gain, mw, w, wo, rb,
    part, recva, red, mod, inv, tabs, bias, hbuf, qb, kv, cown, cslot,
    mwin, lwin, owin, attn, own, acc,
    in_sem, a_sem, bs_sem, br_sem, zs_sem, zr_sem, f_sem, ys_sem, yr_sem, h_sem, os_sem, or_sem,
):
    s = lax.axis_index("sp")
    t = lax.axis_index("tp")
    z, y = s // YN, s % YN
    x, c = t // 2, t % 2

    def tp_of(dx, f):
        return lax.rem(x + dx, XN) * 2 + (c if f == 0 else 1 - c)

    tp_peers = [(dx, f) for dx in (2, 1, 3, 0) for f in (0, 1) if (dx, f) != (0, 0)]
    z_order = sorted(range(1, ZN), key=lambda d: -min(d, ZN - d))
    y_order = sorted(range(1, YN), key=lambda d: -min(d, YN - d))

    loads = {}

    def load(name, k, src, dst):
        loads[name] = pltpu.make_async_copy(src, dst, in_sem.at[k])
        loads[name].start()

    load("cond", 0, cond_h, cond)
    load("cctx", 1, cctx_h, cctx)
    load("sc", 2, scw_h, mw.at[0])
    load("sh", 3, shw_h, mw.at[1])
    load("gt", 4, gtw_h, mw.at[2])
    load("ctx", 5, ctx_h, craw.at[0])
    load("rb", 6, rb_h, rb)
    load("gain", 7, gain_h, gain)
    load("lat", 8, lat_h, lat)
    load("qw", 9, qw_h, w.at[:, 0:128])
    load("kw", 10, kw_h, w.at[:, 128:256])
    load("vw", 11, vw_h, w.at[:, 256:384])
    load("ow", 12, ow_h, wo)

    barrier = pltpu.get_barrier_semaphore()

    def hello(sp, tp):
        pl.semaphore_signal(
            barrier, inc=1, device_id={"sp": sp, "tp": tp}, device_id_type=pl.DeviceIdType.MESH
        )

    def sp_z(d):
        return lax.rem(z + d, ZN) * YN + y

    def sp_y(d):
        return z * YN + lax.rem(y + d, YN)

    for d in z_order:
        hello(sp_z(d), t)
    for d in y_order:
        hello(sp_y(d), t)
    for dx, f in tp_peers:
        hello(s, tp_of(dx, f))
    has_next = s < ZN * YN - 1
    has_prev = s > 0
    next_far = jnp.logical_and(y == YN - 1, has_next)
    prev_far = jnp.logical_and(y == 0, has_prev)

    @pl.when(next_far)
    def _():
        hello(s + 1, t)

    @pl.when(prev_far)
    def _():
        hello(s - 1, t)

    def rcopy(src, dst, ssem, rsem, sp, tp):
        return pltpu.make_async_remote_copy(
            src_ref=src, dst_ref=dst, send_sem=ssem, recv_sem=rsem,
            device_id={"sp": sp, "tp": tp}, device_id_type=pl.DeviceIdType.MESH,
        )

    loads["cond"].wait()
    loads["cctx"].wait()

    def silu_row(ref):
        v = jnp.concatenate([ref[pl.ds(2 * t, 1), :], ref[pl.ds(2 * t + 1, 1), :]], axis=1)
        return (v / (1.0 + jnp.exp(-v))).astype(BF16)

    row = lax.broadcasted_iota(jnp.int32, (16, 256), 0)
    act = jnp.where(
        row == 0, silu_row(cond).astype(F32), jnp.where(row == 1, silu_row(cctx).astype(F32), 0.0)
    ).astype(BF16)
    for k, name in enumerate(("sc", "sh", "gt")):
        loads[name].wait()
        for n in range(8):
            o = jnp.dot(act, mw[k, :, n * 256 : (n + 1) * 256], preferred_element_type=F32)
            for i in range(2):
                j = 2 * n + i
                piece = o[:, i * 128 : (i + 1) * 128]
                for r in range(1 if k == 2 else 2):
                    part[j // 8, 2 * k + r, j % 8 : j % 8 + 1, :] = piece[r : r + 1, :]

    pl.semaphore_wait(
        barrier, ZN - 1 + YN - 1 + 2 * XN - 1 + next_far.astype(jnp.int32) + prev_far.astype(jnp.int32)
    )

    a_copy = rcopy(part.at[1 - c], recva, a_sem.at[0], a_sem.at[1], s, tp_of(0, 1))
    a_copy.start()

    loads["ctx"].wait()
    half = pl.ds(pl.multiple_of(c * 1024, 1024), 1024)
    z_copies = [
        rcopy(craw.at[0, :, half], craw.at[ZN - d, :, half], zs_sem.at[d], zr_sem.at[ZN - d], sp_z(d), t)
        for d in z_order
    ]
    for cp in z_copies:
        cp.start()

    a_copy.wait_recv()
    red[0, 0] = part[c] + recva[...]
    b_copies = [
        rcopy(red.at[0, 0], red.at[dx, f], bs_sem.at[2 * dx + f], br_sem.at[2 * dx + f], s, tp_of(dx, f))
        for dx, f in tp_peers
    ]
    for cp in b_copies:
        cp.start()

    loads["rb"].wait()
    full = jnp.concatenate([rb[0], jnp.zeros((15, 97), F32)], axis=1)
    lane = lax.broadcasted_iota(jnp.int32, (15, 128), 1)
    tabs[0] = pltpu.roll(full, 113, 1)
    tabs[1] = pltpu.roll(full, 49, 1)
    lane = lax.broadcasted_iota(jnp.int32, (1, 128), 1)
    qcol = lax.broadcasted_iota(jnp.int32, (GW, 128), 0)
    kcol = lax.broadcasted_iota(jnp.int32, (GW, 128), 1) % GW
    first = jnp.clip(qcol - WC // 2, 0, GW - WC)
    inside = jnp.logical_and(kcol >= first, kcol < first + WC)
    for a in range(14):
        v = jnp.where(
            jnp.logical_and(lane >= 49, lane <= 79), tabs[1, a + 1 : a + 2, :], tabs[0, a : a + 1, :]
        )
        spread = pltpu.roll(jnp.broadcast_to(v, (GW, 128)), 0, 1, stride=1, stride_axis=0)
        bias[a] = jnp.where(inside, spread, NEG)

    loads["lat"].wait()
    for b in range(TOK // 128):
        rows = slice(b * 128, (b + 1) * 128)
        sq = jnp.zeros((128, 128), F32)
        for j in range(NT):
            v = lat[rows, j * 128 : (j + 1) * 128].astype(F32)
            sq += v * v
        mean = jnp.sum(sq, axis=1, keepdims=True) * (1.0 / D)
        inv[rows, :] = jnp.broadcast_to(lax.rsqrt(mean + EPS), (128, 128))

    for cp in z_copies:
        cp.wait_recv()
    f_copy = rcopy(
        craw.at[1:ZN, :, half], craw.at[1:ZN, :, half], f_sem.at[0], f_sem.at[1], s, tp_of(0, 1)
    )
    f_copy.start()

    for cp in b_copies:
        cp.wait_recv()
    loads["gain"].wait()
    for f in range(2):
        tot = red[0, f] + red[1, f] + red[2, f] + red[3, f]
        hh = c if f == 0 else 1 - c
        gn = gain[pl.ds(pl.multiple_of(hh * 8, 8), 8), :]
        mod[hh, 0] = gn * (1.0 + tot[0])
        mod[hh, 1] = gn * (1.0 + tot[1])
        mod[hh, 2] = tot[2]
        mod[hh, 3] = tot[3]
        mod[hh, 4] = tot[4]

    def mrow(v, j):
        return mod[j // 8, v, j % 8 : j % 8 + 1, :]

    for name in ("qw", "kw", "vw"):
        loads[name].wait()

    def project(r0, n):
        rows = slice(r0, r0 + n)
        for j in range(NT):
            cols = slice(j * 128, (j + 1) * 128)
            v = lat[rows, cols].astype(F32) * inv[rows, :] * mrow(0, j) + mrow(2, j)
            hbuf[rows, cols] = v.astype(BF16)
        o = jnp.dot(hbuf[rows, :], w[...], preferred_element_type=F32).astype(BF16)
        qb[rows, :] = o[:, 0:128]
        kv[0, OWN + r0 : OWN + r0 + n, :] = o[:, 128:256]
        kv[1, OWN + r0 : OWN + r0 + n, :] = o[:, 256:384]

    project(TOK - BEFORE * GW, BEFORE * GW)
    to_next = rcopy(
        kv.at[:, KVN - (BEFORE + AFTER) * GW : KVN - AFTER * GW, :], kv.at[:, 0:OWN, :],
        h_sem.at[0], h_sem.at[1], s + 1, t,
    )

    @pl.when(has_next)
    def _():
        to_next.start()

    project(0, BEFORE * GW)
    to_prev = rcopy(
        kv.at[:, OWN : OWN + AFTER * GW, :], kv.at[:, KVN - AFTER * GW : KVN, :],
        h_sem.at[2], h_sem.at[3], s - 1, t,
    )

    @pl.when(has_prev)
    def _():
        to_prev.start()

    f_copy.wait_recv()
    sq = jnp.zeros((CB, 128), F32)
    for j in range(NT):
        v = craw[:, :, j * 128 : (j + 1) * 128].astype(F32).reshape(CB, 128)
        sq += v * v
    cinv = lax.rsqrt(jnp.sum(sq, axis=1, keepdims=True) * (1.0 / D) + EPS)
    cinv = jnp.broadcast_to(cinv, (CB, 128))
    for j in range(NT):
        cols = slice(j * 128, (j + 1) * 128)
        v = craw[:, :, cols].astype(F32).reshape(CB, 128)
        hbuf[TOK : TOK + CB, cols] = (v * cinv * mrow(1, j) + mrow(3, j)).astype(BF16)
    o = jnp.dot(hbuf[TOK : TOK + CB, :], w[:, 128:384], preferred_element_type=F32).astype(BF16)
    cslot[0, 0] = o[:, 0:128]
    cslot[0, 1] = o[:, 128:256]
    y_copies = [
        rcopy(cslot.at[0], cslot.at[YN - d], ys_sem.at[d], yr_sem.at[YN - d], sp_y(d), t)
        for d in y_order
    ]
    for cp in y_copies:
        cp.start()

    project(BEFORE * GW, TOK - 2 * BEFORE * GW)

    factor = HD ** (-0.5)
    base = s * ROWS

    def window(r):
        g = base + r
        first_row = jnp.clip(g - WR // 2, 0, ALL_ROWS - WR)
        a0 = first_row - g + WR - 1
        k0 = pl.multiple_of((first_row - base + BEFORE) * GW, GW)
        rows = slice(r * GW, (r + 1) * GW)
        keys = kv[0, pl.ds(k0, WR * GW), :]
        vals = kv[1, pl.ds(k0, WR * GW), :]
        sc = lax.dot_general(qb[rows, :], keys, NT_DIMS, preferred_element_type=F32) * factor
        sc = jnp.concatenate(
            [sc[:, i * 128 : (i + 1) * 128] + bias[a0 + 2 * i] for i in range(WR // 2)], axis=1
        )
        m = jnp.max(sc, axis=1, keepdims=True)
        p = jnp.exp(sc - m)
        mwin[rows, :] = jnp.broadcast_to(m, (GW, 128))
        lwin[rows, :] = jnp.broadcast_to(jnp.sum(p, axis=1, keepdims=True), (GW, 128))
        owin[rows, :] = jnp.dot(p.astype(BF16), vals, preferred_element_type=F32)

    for r in range(BEFORE, ROWS - AFTER):
        window(r)

    @pl.when(has_prev)
    def _():
        to_next.wait_recv()

    @pl.when(has_next)
    def _():
        to_prev.wait_recv()

    for r in (*range(BEFORE), *range(ROWS - AFTER, ROWS)):
        window(r)

    for cp in y_copies:
        cp.wait_recv()
    o_copies = {}
    for dx in (2, 1, 3, 0):
        chip = lax.rem(x + dx, XN)
        rows = pl.ds(pl.multiple_of(chip * 160, 160), 160)
        ckeys = cslot[:, 0].reshape(YN * CB, HD)
        cvals = cslot[:, 1].reshape(YN * CB, HD)
        sc = lax.dot_general(qb[rows, :], ckeys, NT_DIMS, preferred_element_type=F32) * factor
        mw_ = mwin[rows, :]
        m = jnp.maximum(jnp.max(sc, axis=1, keepdims=True), mw_)
        p = jnp.concatenate(
            [jnp.exp(sc[:, i * 128 : (i + 1) * 128] - m) for i in range(YN * CB // 128)], axis=1
        )
        alpha = jnp.exp(mw_ - m)
        den = alpha * lwin[rows, :] + jnp.sum(p, axis=1, keepdims=True)
        o = alpha * owin[rows, :] + jnp.dot(p.astype(BF16), cvals, preferred_element_type=F32)
        o = (o / den).astype(BF16)
        attn[2 * dx] = o[0:80]
        attn[2 * dx + 1] = o[80:160]
        for cc in range(2):
            if dx != 0:
                cp = rcopy(
                    attn.at[2 * dx + cc], own.at[2 * dx + c],
                    os_sem.at[2 * dx + cc], or_sem.at[2 * dx + c], s, chip * 2 + cc,
                )
                cp.start()
                o_copies[(dx, cc)] = cp
        if dx == 0:
            cp = rcopy(attn.at[1 - c], own.at[c], os_sem.at[0], or_sem.at[c], s, tp_of(0, 1))
            cp.start()
            o_copies[(0, 1)] = cp
            own[c] = attn[c]

    loads["ow"].wait()
    for n, dx in enumerate((0, 1, 3, 2)):
        for cc in range(2):
            src = own.at[2 * dx + cc]
            if dx == 0:
                if cc == 1:
                    rcopy(
                        attn.at[1 - c], own.at[1 - c], os_sem.at[0], or_sem.at[1 - c], s, tp_of(0, 1)
                    ).wait_recv()
            else:
                rcopy(
                    attn.at[2 * dx + cc], src, os_sem.at[2 * dx + cc], or_sem.at[2 * dx + cc],
                    s, tp_of(dx, 0),
                ).wait_recv()
        lhs = jnp.concatenate([own[2 * dx], own[2 * dx + 1]], axis=1)
        chip = lax.rem(x + XN - dx, XN)
        wrows = pl.ds(pl.multiple_of(chip * 256, 256), 256)
        res = pl.ds(pl.multiple_of(t * 80, 80), 80)
        for q in range(8):
            cols = slice(q * 256, (q + 1) * 256)
            o = jnp.dot(lhs, wo[wrows, cols], preferred_element_type=F32)
            if n > 0:
                o += acc[:, cols]
            if n < 3:
                acc[:, cols] = o
            else:
                for i in range(2):
                    j = 2 * q + i
                    jc = slice(j * 128, (j + 1) * 128)
                    v = lat[res, jc].astype(F32) + mrow(4, j) * o[:, i * 128 : (i + 1) * 128]
                    out_ref[:, jc] = v.astype(BF16)

    a_copy.wait_send()
    f_copy.wait_send()
    for cp in (*z_copies, *b_copies, *y_copies, *o_copies.values()):
        cp.wait_send()

    @pl.when(has_next)
    def _():
        to_next.wait_send()

    @pl.when(has_prev)
    def _():
        to_prev.wait_send()


def shards(
    latents, cond, ctx_cond, context, norm_gain, shift_weight, scale_weight, gate_weight,
    q_weight, k_weight, v_weight, out_weight, rel_bias,
):
    dma = pltpu.SemaphoreType.DMA
    scratch = [
        pltpu.VMEM((TOK, D), BF16),
        pltpu.VMEM((NT, 128), F32),
        pltpu.VMEM((NT, 128), F32),
        pltpu.VMEM((ZN, CR, D), BF16),
        pltpu.VMEM((NT, 128), F32),
        pltpu.VMEM((3, 256, D), BF16),
        pltpu.VMEM((D, 384), BF16),
        pltpu.VMEM((1024, D), BF16),
        pltpu.VMEM((1, 15, 31), F32),
        pltpu.VMEM((2, 5, 8, 128), F32),
        pltpu.VMEM((5, 8, 128), F32),
        pltpu.VMEM((XN, 2, 5, 8, 128), F32),
        pltpu.VMEM((2, 5, 8, 128), F32),
        pltpu.VMEM((TOK, 128), F32),
        pltpu.VMEM((2, 15, 128), F32),
        pltpu.VMEM((14, GW, 128), F32),
        pltpu.VMEM((TOK + CB, D), BF16),
        pltpu.VMEM((TOK, HD), BF16),
        pltpu.VMEM((2, KVN, HD), BF16),
        pltpu.VMEM((2, CB, HD), BF16),
        pltpu.VMEM((YN, 2, CB, HD), BF16),
        pltpu.VMEM((TOK, HD), F32),
        pltpu.VMEM((TOK, HD), F32),
        pltpu.VMEM((TOK, HD), F32),
        pltpu.VMEM((8, 80, HD), BF16),
        pltpu.VMEM((8, 80, HD), BF16),
        pltpu.VMEM((80, D), F32),
        dma((13,)), dma((2,)), dma((8,)), dma((8,)), dma((ZN,)), dma((ZN,)), dma((2,)),
        dma((YN,)), dma((YN,)), dma((4,)), dma((8,)), dma((8,)),
    ]
    anyspec = pl.BlockSpec(memory_space=pl.ANY)
    return pl.pallas_call(
        body,
        out_shape=jax.ShapeDtypeStruct((80, D), BF16),
        in_specs=[anyspec] * 13,
        out_specs=pl.BlockSpec(memory_space=pltpu.VMEM),
        scratch_shapes=scratch,
        compiler_params=pltpu.CompilerParams(
            collective_id=0, has_side_effects=True, vmem_limit_bytes=56 * 1024 * 1024
        ),
        name="step",
    )(
        latents, cond.reshape(NT, 128), ctx_cond.reshape(NT, 128), context, norm_gain.reshape(NT, 128),
        shift_weight, scale_weight, gate_weight, q_weight, k_weight, v_weight, out_weight, rel_bias,
    )


def solution(mesh):
    in_specs = (
        P("sp", None),
        P(),
        P(),
        P("sp", None),
        P(),
        P("tp", None),
        P("tp", None),
        P("tp", None),
        P(None, "tp"),
        P(None, "tp"),
        P(None, "tp"),
        P(),
        P("tp", None, None),
    )
    out_specs = P(("sp", "tp"), None)
    return jax.shard_map(shards, mesh=mesh, in_specs=in_specs, out_specs=out_specs, check_vma=False)
```

```python
import jax
import jax.numpy as jnp
from jax import lax
from jax.experimental import pallas as pl
from jax.experimental.pallas import tpu as pltpu
from jax.sharding import PartitionSpec as P

D = 2048
HD = 128
GW = 64
WR = 8
WC = 16
EPS = 1e-06
NEG = -1e30
ZN, YN, XN = 12, 8, 4
NT = D // 128
TOK = 640
ROWS = TOK // GW
ALL_ROWS = ROWS * ZN * YN
BEFORE, AFTER = 4, 3
OWN = BEFORE * GW
KVN = (BEFORE + ROWS + AFTER) * GW
CR = 8
NEAR = (0, 1, 2, 3, 4, 11, 10, 9)
FAR = (5, 6, 7, 8)
NB, FB = CR * len(NEAR), CR * len(FAR)
F32 = jnp.float32
BF16 = jnp.bfloat16
NT_DIMS = (((1,), (1,)), ((), ()))


def body(
    lat_h, cond_h, cctx_h, ctx_h, gain_h, shw_h, scw_h, gtw_h, qw_h, kw_h, vw_h, ow_h, rb_h,
    out_ref,
    lat, cond, cctx, craw, gain, mw, w, wo, rb,
    part, recva, red, mod, inv, bias, hbuf, qb, kv, kown, farin, kvn, kvf,
    mwin, lwin, owin, attn, own, acc,
    in_sem, a_sem, bs_sem, br_sem, zs_sem, zr_sem, f_sem, ys_sem, yr_sem, ws_sem, wr_sem, vs_sem, vr_sem, far_sem, h_sem, os_sem, or_sem,
):
    s = lax.axis_index("sp")
    t = lax.axis_index("tp")
    z, y = s // YN, s % YN
    x, c = t // 2, t % 2

    def tp_of(dx, f):
        return lax.rem(x + dx, XN) * 2 + (c if f == 0 else 1 - c)

    tp_peers = [(dx, f) for dx in (2, 1, 3, 0) for f in (0, 1) if (dx, f) != (0, 0)]
    def by_hops(offsets):
        return sorted(offsets, key=lambda d: -min(d, ZN - d))

    raw_order = by_hops((-o) % ZN for o in NEAR[1:])
    far_order = by_hops((-o) % ZN for o in FAR)
    meet_order = by_hops((1, 2, 3, 4, 8, 9, 10, 11))
    y_order = sorted(range(1, YN), key=lambda d: -min(d, YN - d))

    scope = []

    def phase(name):
        while scope:
            scope.pop().__exit__(None, None, None)
        if name:
            scope.append(jax.named_scope(name))
            scope[0].__enter__()

    barrier = pltpu.get_barrier_semaphore()

    def hello(sp, tp):
        pl.semaphore_signal(
            barrier, inc=1, device_id={"sp": sp, "tp": tp}, device_id_type=pl.DeviceIdType.MESH
        )

    def sp_z(d):
        return lax.rem(z + d, ZN) * YN + y

    def sp_y(d):
        return z * YN + lax.rem(y + d, YN)

    for d in meet_order:
        hello(sp_z(d), t)
    for d in y_order:
        hello(sp_y(d), t)
    for dx, f in tp_peers:
        hello(s, tp_of(dx, f))
    has_next = s < ZN * YN - 1
    has_prev = s > 0
    next_far = jnp.logical_and(y == YN - 1, has_next)
    prev_far = jnp.logical_and(y == 0, has_prev)

    @pl.when(next_far)
    def _():
        hello(s + 1, t)

    @pl.when(prev_far)
    def _():
        hello(s - 1, t)

    loads = {}

    def load(name, k, src, dst):
        loads[name] = pltpu.make_async_copy(src, dst, in_sem.at[k])
        loads[name].start()

    load("ctx", 5, ctx_h, craw.at[0])
    load("cond", 0, cond_h, cond)
    load("cctx", 1, cctx_h, cctx)
    load("sc", 2, scw_h, mw.at[0])
    load("sh", 3, shw_h, mw.at[1])
    load("rb", 6, rb_h, rb)
    load("gain", 7, gain_h, gain)
    load("gt", 4, gtw_h, mw.at[2])
    load("lat", 8, lat_h, lat)
    load("qw", 9, qw_h, w.at[:, 0:128])
    load("kw", 10, kw_h, w.at[:, 128:256])
    load("vw", 11, vw_h, w.at[:, 256:384])
    load("ow", 12, ow_h, wo)

    def rcopy(src, dst, ssem, rsem, sp, tp):
        return pltpu.make_async_remote_copy(
            src_ref=src, dst_ref=dst, send_sem=ssem, recv_sem=rsem,
            device_id={"sp": sp, "tp": tp}, device_id_type=pl.DeviceIdType.MESH,
        )

    loads["cond"].wait()
    loads["cctx"].wait()

    def silu_row(ref):
        v = jnp.concatenate([ref[pl.ds(2 * t, 1), :], ref[pl.ds(2 * t + 1, 1), :]], axis=1)
        return (v / (1.0 + jnp.exp(-v))).astype(BF16)

    half = pl.ds(pl.multiple_of(c * 1024, 1024), 1024)
    z_copies = [
        rcopy(
            craw.at[0, :, half], craw.at[NEAR.index(ZN - d), :, half], zs_sem.at[d], zr_sem.at[ZN - d],
            sp_z(d), t,
        )
        for d in raw_order
    ]

    def meet():
        with jax.named_scope("meet"):
            loads["ctx"].wait()
            pl.semaphore_wait(
                barrier,
                len(meet_order) + YN - 1 + 2 * XN - 1 + next_far.astype(jnp.int32) + prev_far.astype(jnp.int32),
            )
            for cp in z_copies:
                cp.start()
            for i, d in enumerate((3, ZN - 3)):
                pl.semaphore_signal(
                    far_sem.at[i], inc=1, device_id={"sp": sp_z(d), "tp": t},
                    device_id_type=pl.DeviceIdType.MESH,
                )

    late = jnp.logical_and(z >= 7, y >= 4)

    @pl.when(late)
    def _():
        meet()

    def act_rows():
        row = lax.broadcasted_iota(jnp.int32, (16, 256), 0)
        return jnp.where(
            row == 0,
            silu_row(cond).astype(F32),
            jnp.where(row == 1, silu_row(cctx).astype(F32), 0.0),
        ).astype(BF16)

    def partial(k, name):
        act = act_rows()
        loads[name].wait()
        for n in range(8):
            o = jnp.dot(act, mw[k, :, n * 256 : (n + 1) * 256], preferred_element_type=F32)
            for i in range(2):
                j = 2 * n + i
                piece = o[:, i * 128 : (i + 1) * 128]
                for r in range(1 if k == 2 else 2):
                    part[j // 8, 2 * k + r, j % 8 : j % 8 + 1, :] = piece[r : r + 1, :]

    with jax.named_scope("partials"):
        partial(0, "sc")
        partial(1, "sh")

    @pl.when(jnp.logical_not(late))
    def _():
        meet()

    vec, gate = slice(0, 4), slice(4, 5)
    a_copy = rcopy(part.at[1 - c, vec], recva.at[vec], a_sem.at[0], a_sem.at[1], s, tp_of(0, 1))
    g_copy = rcopy(part.at[1 - c, gate], recva.at[gate], a_sem.at[2], a_sem.at[3], s, tp_of(0, 1))
    a_copy.start()
    with jax.named_scope("gatepart"):
        partial(2, "gt")
    g_copy.start()
    with jax.named_scope("await_a"):
        a_copy.wait_recv()
    red[0, 0, vec] = part[c, vec] + recva[vec]
    b_copies = [
        rcopy(
            red.at[0, 0, vec], red.at[dx, f, vec], bs_sem.at[2 * dx + f], br_sem.at[2 * dx + f],
            s, tp_of(dx, f),
        )
        for dx, f in tp_peers
    ]
    g_copies = [
        rcopy(
            red.at[0, 0, gate], red.at[dx, f, gate], bs_sem.at[8 + 2 * dx + f],
            br_sem.at[8 + 2 * dx + f], s, tp_of(dx, f),
        )
        for dx, f in tp_peers
    ]
    for cp in b_copies:
        cp.start()

    phase("bias")
    loads["rb"].wait()
    rb_rows = [jnp.concatenate([rb[a], jnp.zeros((1, 97), F32)], axis=1) for a in range(15)]
    lane = lax.broadcasted_iota(jnp.int32, (1, 128), 1)
    qcol = lax.broadcasted_iota(jnp.int32, (GW, 128), 0)
    kcol = lax.broadcasted_iota(jnp.int32, (GW, 128), 1) % GW
    first = jnp.clip(qcol - WC // 2, 0, GW - WC)
    inside = jnp.logical_and(kcol >= first, kcol < first + WC)
    for a in range(14):
        v = jnp.where(
            jnp.logical_and(lane >= 49, lane <= 79),
            pltpu.roll(rb_rows[a + 1], 49, 1),
            pltpu.roll(rb_rows[a], 113, 1),
        )
        spread = pltpu.roll(jnp.broadcast_to(v, (GW, 128)), 0, 1, stride=1, stride_axis=0)
        bias[a] = jnp.where(inside, spread, NEG)

    phase("rms")
    loads["lat"].wait()
    for b in range(TOK // 128):
        rows = slice(b * 128, (b + 1) * 128)
        sq = jnp.zeros((128, 128), F32)
        for j in range(NT):
            v = lat[rows, j * 128 : (j + 1) * 128].astype(F32)
            sq += v * v
        mean = jnp.sum(sq, axis=1, keepdims=True) * (1.0 / D)
        inv[rows, :] = jnp.broadcast_to(lax.rsqrt(mean + EPS), (128, 128))

    phase("send_g")
    g_copy.wait_recv()
    red[0, 0, gate] = part[c, gate] + recva[gate]
    for cp in g_copies:
        cp.start()
    with jax.named_scope("await_b"):
        for cp in b_copies:
            cp.wait_recv()
    loads["gain"].wait()
    for f in range(2):
        tot = red[0, f, vec] + red[1, f, vec] + red[2, f, vec] + red[3, f, vec]
        hh = c if f == 0 else 1 - c
        gn = gain[pl.ds(pl.multiple_of(hh * 8, 8), 8), :]
        mod[hh, 0] = gn * (1.0 + tot[0])
        mod[hh, 1] = gn * (1.0 + tot[1])
        mod[hh, 2] = tot[2]
        mod[hh, 3] = tot[3]

    def mrow(v, j):
        return mod[j // 8, v, j % 8 : j % 8 + 1, :]

    for name in ("qw", "kw", "vw"):
        loads[name].wait()

    def project(r0, n):
        rows = slice(r0, r0 + n)
        for j in range(NT):
            cols = slice(j * 128, (j + 1) * 128)
            v = lat[rows, cols].astype(F32) * inv[rows, :] * mrow(0, j) + mrow(2, j)
            hbuf[rows, cols] = v.astype(BF16)
        o = jnp.dot(hbuf[rows, :], w[...], preferred_element_type=F32).astype(BF16)
        qb[rows, :] = o[:, 0:128]
        kv[0, OWN + r0 : OWN + r0 + n, :] = o[:, 128:256]
        kv[1, OWN + r0 : OWN + r0 + n, :] = o[:, 256:384]

    phase("own_kv")
    def ctx_rows(n, at):
        sq = jnp.zeros((n, 128), F32)
        for j in range(NT):
            v = craw[0 : n // CR, :, j * 128 : (j + 1) * 128].astype(F32).reshape(n, 128)
            sq += v * v
        cinv = lax.rsqrt(jnp.sum(sq, axis=1, keepdims=True) * (1.0 / D) + EPS)
        cinv = jnp.broadcast_to(cinv, (n, 128))
        for j in range(NT):
            cols = slice(j * 128, (j + 1) * 128)
            v = craw[0 : n // CR, :, cols].astype(F32).reshape(n, 128)
            hbuf[at : at + n, cols] = (v * cinv * mrow(1, j) + mrow(3, j)).astype(BF16)

    hbuf[TOK + NB : TOK + NB + 16, :] = jnp.zeros((16, D), BF16)
    ctx_rows(CR, TOK + NB)
    o = jnp.dot(hbuf[TOK + NB : TOK + NB + 16, :], w[:, 128:384], preferred_element_type=F32)
    for i in range(2):
        kown[i] = o[0:CR, i * 128 : (i + 1) * 128].astype(BF16)
    for i in range(2):
        pl.semaphore_wait(far_sem.at[i], 1)
    v_copies = [
        rcopy(
            kown, farin.at[FAR.index(ZN - d)], vs_sem.at[FAR.index(ZN - d)],
            vr_sem.at[FAR.index(ZN - d)], sp_z(d), t,
        )
        for d in far_order
    ]
    for cp in v_copies:
        cp.start()

    phase("proj_edge")
    project(TOK - BEFORE * GW, BEFORE * GW)
    to_next = rcopy(
        kv.at[:, KVN - (BEFORE + AFTER) * GW : KVN - AFTER * GW, :], kv.at[:, 0:OWN, :],
        h_sem.at[0], h_sem.at[1], s + 1, t,
    )

    @pl.when(has_next)
    def _():
        to_next.start()

    project(0, BEFORE * GW)
    to_prev = rcopy(
        kv.at[:, OWN : OWN + AFTER * GW, :], kv.at[:, KVN - AFTER * GW : KVN, :],
        h_sem.at[2], h_sem.at[3], s - 1, t,
    )

    @pl.when(has_prev)
    def _():
        to_prev.start()

    phase("fwd")
    with jax.named_scope('await_z'):
        for cp in z_copies:
            cp.wait_recv()
    f_copy = rcopy(
        craw.at[1:, :, half], craw.at[1:, :, half], f_sem.at[0], f_sem.at[1], s, tp_of(0, 1)
    )
    f_copy.start()

    phase("proj_mid")
    project(BEFORE * GW, TOK - 2 * BEFORE * GW)

    factor = HD ** (-0.5)
    base = s * ROWS

    def window(r):
        g = base + r
        first_row = jnp.clip(g - WR // 2, 0, ALL_ROWS - WR)
        a0 = first_row - g + WR - 1
        k0 = pl.multiple_of((first_row - base + BEFORE) * GW, GW)
        rows = slice(r * GW, (r + 1) * GW)
        keys = kv[0, pl.ds(k0, WR * GW), :]
        vals = kv[1, pl.ds(k0, WR * GW), :]
        sc = lax.dot_general(qb[rows, :], keys, NT_DIMS, preferred_element_type=F32) * factor
        sc = jnp.concatenate(
            [sc[:, i * 128 : (i + 1) * 128] + bias[a0 + 2 * i] for i in range(WR // 2)], axis=1
        )
        m = jnp.max(sc, axis=1, keepdims=True)
        p = jnp.exp(sc - m)
        mwin[rows, :] = jnp.broadcast_to(m, (GW, 128))
        lwin[rows, :] = jnp.broadcast_to(jnp.sum(p, axis=1, keepdims=True), (GW, 128))
        owin[rows, :] = jnp.dot(p.astype(BF16), vals, preferred_element_type=F32)

    phase("ctx_kv")
    f_copy.wait_recv()
    ctx_rows(NB, TOK)
    o = jnp.dot(hbuf[TOK : TOK + NB, :], w[:, 128:384], preferred_element_type=F32)
    for i in range(2):
        kvn[0, i] = o[:, i * 128 : (i + 1) * 128].astype(BF16)
    y_copies = [
        rcopy(kvn.at[0], kvn.at[YN - d], ys_sem.at[d], yr_sem.at[YN - d], sp_y(d), t)
        for d in y_order
    ]
    for cp in y_copies:
        cp.start()

    phase("win_mid")
    for r in range(BEFORE, ROWS - AFTER):
        window(r)

    phase("await_halo")

    @pl.when(has_prev)
    def _():
        to_next.wait_recv()

    @pl.when(has_next)
    def _():
        to_prev.wait_recv()

    phase("win_edge")
    for r in (*range(BEFORE), *range(ROWS - AFTER, ROWS)):
        window(r)

    phase("await_far")
    for cp in v_copies:
        cp.wait_recv()
    for i in range(2):
        kvf[0, i] = farin[:, i].astype(F32).reshape(FB, HD).astype(BF16)
    w_copies = [
        rcopy(kvf.at[0], kvf.at[YN - d], ws_sem.at[d], wr_sem.at[YN - d], sp_y(d), t)
        for d in y_order
    ]
    for cp in w_copies:
        cp.start()

    def merge(rows, ctx):
        ckeys = ctx[:, 0].reshape(-1, HD)
        cvals = ctx[:, 1].reshape(-1, HD)
        sc = lax.dot_general(qb[rows, :], ckeys, NT_DIMS, preferred_element_type=F32) * factor
        m0 = mwin[rows, :]
        m = jnp.maximum(jnp.max(sc, axis=1, keepdims=True), m0)
        p = jnp.concatenate(
            [jnp.exp(sc[:, i * 128 : (i + 1) * 128] - m) for i in range(sc.shape[1] // 128)], axis=1
        )
        alpha = jnp.exp(m0 - m)
        den = alpha * lwin[rows, :] + jnp.sum(p, axis=1, keepdims=True)
        o = alpha * owin[rows, :] + jnp.dot(p.astype(BF16), cvals, preferred_element_type=F32)
        return m, den, o

    phase("await_y")
    for cp in y_copies:
        cp.wait_recv()
    phase("ctx_near")
    for b in range(4):
        rows = slice(b * 160, (b + 1) * 160)
        mwin[rows, :], lwin[rows, :], owin[rows, :] = merge(rows, kvn)
    phase("await_w")
    for cp in w_copies:
        cp.wait_recv()
    phase("ctx_attn")
    o_copies = {}
    for dx in (2, 1, 3, 0):
        chip = lax.rem(x + dx, XN)
        rows = pl.ds(pl.multiple_of(chip * 160, 160), 160)
        _, den, o = merge(rows, kvf)
        o = (o / den).astype(BF16)
        attn[2 * dx] = o[0:80]
        attn[2 * dx + 1] = o[80:160]
        for cc in range(2):
            if dx != 0:
                cp = rcopy(
                    attn.at[2 * dx + cc], own.at[2 * dx + c],
                    os_sem.at[2 * dx + cc], or_sem.at[2 * dx + c], s, chip * 2 + cc,
                )
                cp.start()
                o_copies[(dx, cc)] = cp
        if dx == 0:
            cp = rcopy(attn.at[1 - c], own.at[c], os_sem.at[0], or_sem.at[c], s, tp_of(0, 1))
            cp.start()
            o_copies[(0, 1)] = cp
            own[c] = attn[c]

    phase("out_proj")
    with jax.named_scope("await_g"):
        for cp in g_copies:
            cp.wait_recv()
    for f in range(2):
        hh = c if f == 0 else 1 - c
        mod[hh, 4] = red[0, f, 4] + red[1, f, 4] + red[2, f, 4] + red[3, f, 4]
    loads["ow"].wait()
    for n, dx in enumerate((0, 1, 3, 2)):
        for cc in range(2):
            src = own.at[2 * dx + cc]
            if dx == 0:
                if cc == 1:
                    rcopy(
                        attn.at[1 - c], own.at[1 - c], os_sem.at[0], or_sem.at[1 - c], s, tp_of(0, 1)
                    ).wait_recv()
            else:
                rcopy(
                    attn.at[2 * dx + cc], src, os_sem.at[2 * dx + cc], or_sem.at[2 * dx + cc],
                    s, tp_of(dx, 0),
                ).wait_recv()
        lhs = jnp.concatenate([own[2 * dx], own[2 * dx + 1]], axis=1)
        chip = lax.rem(x + XN - dx, XN)
        wrows = pl.ds(pl.multiple_of(chip * 256, 256), 256)
        res = pl.ds(pl.multiple_of(t * 80, 80), 80)
        for q in range(8):
            cols = slice(q * 256, (q + 1) * 256)
            o = jnp.dot(lhs, wo[wrows, cols], preferred_element_type=F32)
            if n > 0:
                o += acc[:, cols]
            if n < 3:
                acc[:, cols] = o
            else:
                for i in range(2):
                    j = 2 * q + i
                    jc = slice(j * 128, (j + 1) * 128)
                    v = lat[res, jc].astype(F32) + mrow(4, j) * o[:, i * 128 : (i + 1) * 128]
                    out_ref[:, jc] = v.astype(BF16)

    phase("drain")
    a_copy.wait_send()
    f_copy.wait_send()
    g_copy.wait_send()
    for cp in (*z_copies, *b_copies, *g_copies, *v_copies, *y_copies, *w_copies, *o_copies.values()):
        cp.wait_send()

    @pl.when(has_next)
    def _():
        to_next.wait_send()

    @pl.when(has_prev)
    def _():
        to_prev.wait_send()

    phase(None)


def shards(
    latents, cond, ctx_cond, context, norm_gain, shift_weight, scale_weight, gate_weight,
    q_weight, k_weight, v_weight, out_weight, rel_bias,
):
    dma = pltpu.SemaphoreType.DMA
    scratch = [
        pltpu.VMEM((TOK, D), BF16),
        pltpu.VMEM((NT, 128), F32),
        pltpu.VMEM((NT, 128), F32),
        pltpu.VMEM((len(NEAR), CR, D), BF16),
        pltpu.VMEM((NT, 128), F32),
        pltpu.VMEM((3, 256, D), BF16),
        pltpu.VMEM((D, 384), BF16),
        pltpu.VMEM((1024, D), BF16),
        pltpu.VMEM((15, 1, 31), F32),
        pltpu.VMEM((2, 5, 8, 128), F32),
        pltpu.VMEM((5, 8, 128), F32),
        pltpu.VMEM((XN, 2, 5, 8, 128), F32),
        pltpu.VMEM((2, 5, 8, 128), F32),
        pltpu.VMEM((TOK, 128), F32),
        pltpu.VMEM((14, GW, 128), F32),
        pltpu.VMEM((TOK + NB + 16, D), BF16),
        pltpu.VMEM((TOK, HD), BF16),
        pltpu.VMEM((2, KVN, HD), BF16),
        pltpu.VMEM((2, CR, HD), BF16),
        pltpu.VMEM((len(FAR), 2, CR, HD), BF16),
        pltpu.VMEM((YN, 2, NB, HD), BF16),
        pltpu.VMEM((YN, 2, FB, HD), BF16),
        pltpu.VMEM((TOK, HD), F32),
        pltpu.VMEM((TOK, HD), F32),
        pltpu.VMEM((TOK, HD), F32),
        pltpu.VMEM((8, 80, HD), BF16),
        pltpu.VMEM((8, 80, HD), BF16),
        pltpu.VMEM((80, D), F32),
        dma((13,)), dma((4,)), dma((16,)), dma((16,)), dma((ZN,)), dma((ZN,)), dma((2,)),
        dma((YN,)), dma((YN,)), dma((YN,)), dma((YN,)), dma((4,)), dma((4,)),
        pltpu.SemaphoreType.REGULAR((2,)), dma((4,)), dma((8,)), dma((8,)),
    ]
    anyspec = pl.BlockSpec(memory_space=pl.ANY)
    operands = (
        latents, cond.reshape(NT, 128), ctx_cond.reshape(NT, 128), context, norm_gain.reshape(NT, 128),
        shift_weight, scale_weight, gate_weight, q_weight, k_weight, v_weight, out_weight,
        rel_bias.transpose(1, 0, 2),
    )
    return pl.pallas_call(
        body,
        out_shape=jax.ShapeDtypeStruct((80, D), BF16),
        in_specs=[anyspec] * len(operands),
        out_specs=pl.BlockSpec(memory_space=pltpu.VMEM),
        scratch_shapes=scratch,
        compiler_params=pltpu.CompilerParams(
            collective_id=0, has_side_effects=True, vmem_limit_bytes=40 * 1024 * 1024
        ),
        name="step",
    )(*(pltpu.with_memory_space_constraint(v, pltpu.HBM) for v in operands))


def solution(mesh):
    in_specs = (
        P("sp", None),
        P(),
        P(),
        P("sp", None),
        P(),
        P("tp", None),
        P("tp", None),
        P("tp", None),
        P(None, "tp"),
        P(None, "tp"),
        P(None, "tp"),
        P(),
        P("tp", None, None),
    )
    out_specs = P(("sp", "tp"), None)
    return jax.shard_map(shards, mesh=mesh, in_specs=in_specs, out_specs=out_specs, check_vma=False)
```

```python
import jax
import jax.numpy as jnp
from jax import lax
from jax.experimental import pallas as pl
from jax.experimental.pallas import tpu as pltpu
from jax.sharding import PartitionSpec as P

D = 2048
HD = 128
GW = 64
WR = 8
WC = 16
EPS = 1e-06
NEG = -1e30
ZN, YN, XN = 12, 8, 4
NT = D // 128
TOK = 640
ROWS = TOK // GW
ALL_ROWS = ROWS * ZN * YN
BEFORE, AFTER = 4, 3
OWN = BEFORE * GW
KVN = (BEFORE + ROWS + AFTER) * GW
CR = 8
NEAR = (0, 1, 2, 3, 4, 11, 10, 9)
FAR = (5, 6, 7, 8)
NB, FB = CR * len(NEAR), CR * len(FAR)
YH = YN // 2
ZB = CR * YH
F32 = jnp.float32
BF16 = jnp.bfloat16
NT_DIMS = (((1,), (1,)), ((), ()))


def body(
    lat_h, cond_h, cctx_h, ctx_h, gain_h, shw_h, scw_h, gtw_h, qw_h, kw_h, vw_h, ow_h, rb_h,
    out_ref,
    lat, cond, cctx, craw, gain, mw, w, wo, rb,
    part, recva, red, redg, mod, inv, bias, hbuf, qb, kv, kown, farin, kvn, kvf, kvz, yraw,
    mwin, lwin, owin, attn, own, acc,
    in_sem, a_sem, b_sem, z_sem, f_sem, ys_sem, yr_sem, ws_sem, wr_sem, v_sem, far_sem, u_sem, ur_sem,
    fs_sem, fr_sem, k_sem, h_sem, o_sem, or_sem,
):
    s = lax.axis_index("sp")
    t = lax.axis_index("tp")
    z, y = s // YN, s % YN
    x, c = t // 2, t % 2
    yi = y // 2
    even, odd = y % 2 == 0, y % 2 == 1

    def tp_of(dx, f):
        return lax.rem(x + dx, XN) * 2 + (c if f == 0 else 1 - c)

    tp_peers = [(dx, f) for dx in (2, 1, 3, 0) for f in (0, 1) if (dx, f) != (0, 0)]
    def by_hops(offsets):
        return sorted(offsets, key=lambda d: -min(d, ZN - d))

    raw_order = by_hops((-o) % ZN for o in NEAR[1:])
    far_order = by_hops((-o) % ZN for o in FAR)
    meet_order = by_hops((1, 2, 3, 4, 8, 9, 10, 11))
    y_order = sorted(range(1, YN), key=lambda d: -min(d, YN - d))

    scope = []

    def phase(name):
        while scope:
            scope.pop().__exit__(None, None, None)
        if name:
            scope.append(jax.named_scope(name))
            scope[0].__enter__()

    phase("hello")
    barrier = pltpu.get_barrier_semaphore()

    def hello(sp, tp):
        pl.semaphore_signal(
            barrier, inc=1, device_id={"sp": sp, "tp": tp}, device_id_type=pl.DeviceIdType.MESH
        )

    def sp_z(d):
        return lax.rem(z + d, ZN) * YN + y

    def sp_y(d):
        return z * YN + lax.rem(y + d, YN)

    for d in meet_order:
        hello(sp_z(d), t)
    for d in y_order:
        hello(sp_y(d), t)
    for dx, f in tp_peers:
        hello(s, tp_of(dx, f))
    has_next = s < ZN * YN - 1
    has_prev = s > 0
    next_far = jnp.logical_and(y == YN - 1, has_next)
    prev_far = jnp.logical_and(y == 0, has_prev)

    @pl.when(next_far)
    def _():
        hello(s + 1, t)

    @pl.when(prev_far)
    def _():
        hello(s - 1, t)

    loads = {}

    def load(name, k, src, dst):
        loads[name] = pltpu.make_async_copy(src, dst, in_sem.at[k])
        loads[name].start()

    load("ctx", 5, ctx_h, craw.at[0])
    own_row = pltpu.make_async_copy(ctx_h, yraw.at[yi], in_sem.at[13])

    @pl.when(even)
    def _():
        own_row.start()

    load("cond", 0, cond_h, cond)
    load("cctx", 1, cctx_h, cctx)
    load("sc", 2, scw_h, mw.at[0])
    load("sh", 3, shw_h, mw.at[1])
    load("rb", 6, rb_h, rb)
    load("gain", 7, gain_h, gain)
    load("gt", 4, gtw_h, mw.at[2])
    load("lat", 8, lat_h, lat)
    load("qw", 9, qw_h, w.at[:, 0:128])
    load("kw", 10, kw_h, w.at[:, 128:256])
    load("vw", 11, vw_h, w.at[:, 256:384])
    load("ow", 12, ow_h, wo)

    def rcopy(src, dst, ssem, rsem, sp, tp):
        return pltpu.make_async_remote_copy(
            src_ref=src, dst_ref=dst, send_sem=ssem, recv_sem=rsem,
            device_id={"sp": sp, "tp": tp}, device_id_type=pl.DeviceIdType.MESH,
        )

    def silu_row(ref):
        v = jnp.concatenate([ref[pl.ds(2 * t, 1), :], ref[pl.ds(2 * t + 1, 1), :]], axis=1)
        return (v / (1.0 + jnp.exp(-v))).astype(BF16)

    half = pl.ds(pl.multiple_of(c * 1024, 1024), 1024)
    z_copies = [
        rcopy(
            craw.at[0, :, half], craw.at[NEAR.index(ZN - d), :, half], z_sem.at[0], z_sem.at[1],
            sp_z(d), t,
        )
        for d in raw_order
    ]

    y_raw = [
        rcopy(craw.at[0, :, half], yraw.at[yi, :, half], u_sem.at[0], ur_sem.at[yi], sp_y(d), t)
        for d in y_order
    ]

    def arrived(ref, sem, i):
        return rcopy(ref, ref, u_sem.at[0], sem.at[i], sp_y(1), t)

    def meet():
        with jax.named_scope("meet"):
            loads["ctx"].wait()
            pl.semaphore_wait(
                barrier,
                len(meet_order) + YN - 1 + 2 * XN - 1 + next_far.astype(jnp.int32) + prev_far.astype(jnp.int32),
            )

            @pl.when(odd)
            def _():
                for cp in z_copies:
                    cp.start()

            @pl.when(even)
            def _():
                for cp in y_raw:
                    cp.start()

            for i, d in enumerate((3, ZN - 3)):
                pl.semaphore_signal(
                    far_sem.at[i], inc=1, device_id={"sp": sp_z(d), "tp": t},
                    device_id_type=pl.DeviceIdType.MESH,
                )

    late = jnp.logical_and(z >= 7, y >= 4)

    @pl.when(late)
    def _():
        meet()

    def act_rows():
        row = lax.broadcasted_iota(jnp.int32, (16, 256), 0)
        return jnp.where(
            row == 0,
            silu_row(cond).astype(F32),
            jnp.where(row == 1, silu_row(cctx).astype(F32), 0.0),
        ).astype(BF16)

    def partial(k, name):
        act = act_rows()
        loads[name].wait()
        for n in range(8):
            o = jnp.dot(act, mw[k, :, n * 256 : (n + 1) * 256], preferred_element_type=F32)
            for i in range(2):
                j = 2 * n + i
                piece = o[:, i * 128 : (i + 1) * 128]
                for r in range(1 if k == 2 else 2):
                    part[j // 8, 2 * k + r, j % 8 : j % 8 + 1, :] = piece[r : r + 1, :]

    with jax.named_scope("partials"):
        loads["cond"].wait()
        loads["cctx"].wait()
        partial(0, "sc")
        partial(1, "sh")

    @pl.when(jnp.logical_not(late))
    def _():
        meet()

    vec, gate = slice(0, 4), slice(4, 5)
    a_copy = rcopy(part.at[1 - c, vec], recva.at[vec], a_sem.at[0], a_sem.at[1], s, tp_of(0, 1))
    g_copy = rcopy(part.at[1 - c, gate], recva.at[gate], a_sem.at[2], a_sem.at[3], s, tp_of(0, 1))
    a_copy.start()
    with jax.named_scope("gatepart"):
        partial(2, "gt")
    g_copy.start()
    with jax.named_scope("await_a"):
        a_copy.wait_recv()
    red[0] = (part[c, vec] + recva[vec]).astype(BF16)
    b_copies = [
        rcopy(
            red.at[0], red.at[2 * dx + f], b_sem.at[0], b_sem.at[1], s, tp_of(dx, f),
        )
        for dx, f in tp_peers
    ]
    g_copies = [
        rcopy(
            redg.at[0], redg.at[2 * dx + f], b_sem.at[2], b_sem.at[3], s, tp_of(dx, f),
        )
        for dx, f in tp_peers
    ]
    for cp in b_copies:
        cp.start()

    def together(ref, sems):
        return rcopy(ref, ref, sems.at[0], sems.at[1], s, tp_of(0, 1))

    b_all = together(red.at[1:], b_sem.at[0:2])
    g_all = together(redg.at[1:], b_sem.at[2:4])
    z_all = together(craw.at[1:, :, half], z_sem)
    u_all = together(craw.at[1:, :, half], u_sem)
    v_all = together(farin, v_sem)
    k_all = together(kvz.at[1:], k_sem)
    o_all = together(attn.at[1:], o_sem)

    phase("bias")
    loads["rb"].wait()
    rb_rows = [jnp.concatenate([rb[a], jnp.zeros((1, 97), F32)], axis=1) for a in range(15)]
    lane = lax.broadcasted_iota(jnp.int32, (1, 128), 1)
    qcol = lax.broadcasted_iota(jnp.int32, (GW, 128), 0)
    kcol = lax.broadcasted_iota(jnp.int32, (GW, 128), 1) % GW
    first = jnp.clip(qcol - WC // 2, 0, GW - WC)
    inside = jnp.logical_and(kcol >= first, kcol < first + WC)
    for a in range(14):
        v = jnp.where(
            jnp.logical_and(lane >= 49, lane <= 79),
            pltpu.roll(rb_rows[a + 1], 49, 1),
            pltpu.roll(rb_rows[a], 113, 1),
        )
        spread = pltpu.roll(jnp.broadcast_to(v, (GW, 128)), 0, 1, stride=1, stride_axis=0)
        bias[a] = jnp.where(inside, spread, NEG)

    phase("rms")
    loads["lat"].wait()
    for b in range(TOK // 128):
        rows = slice(b * 128, (b + 1) * 128)
        sq = jnp.zeros((128, 128), F32)
        for j in range(NT):
            v = lat[rows, j * 128 : (j + 1) * 128].astype(F32)
            sq += v * v
        mean = jnp.sum(sq, axis=1, keepdims=True) * (1.0 / D)
        inv[rows, :] = jnp.broadcast_to(lax.rsqrt(mean + EPS), (128, 128))

    phase("send_g")
    g_copy.wait_recv()
    redg[0] = part[c, 4] + recva[4]
    for cp in g_copies:
        cp.start()
    with jax.named_scope("await_b"):
        b_all.wait_recv()
    loads["gain"].wait()
    for f in range(2):
        tot = sum(red[2 * k + f].astype(F32) for k in range(XN))
        hh = c if f == 0 else 1 - c
        gn = gain[pl.ds(pl.multiple_of(hh * 8, 8), 8), :]
        mod[hh, 0] = gn * (1.0 + tot[0])
        mod[hh, 1] = gn * (1.0 + tot[1])
        mod[hh, 2] = tot[2]
        mod[hh, 3] = tot[3]

    def mrow(v, j):
        return mod[j // 8, v, j % 8 : j % 8 + 1, :]

    for name in ("qw", "kw", "vw"):
        loads[name].wait()

    def project(r0, n):
        rows = slice(r0, r0 + n)
        for j in range(NT):
            cols = slice(j * 128, (j + 1) * 128)
            v = lat[rows, cols].astype(F32) * inv[rows, :] * mrow(0, j) + mrow(2, j)
            hbuf[rows, cols] = v.astype(BF16)
        o = jnp.dot(hbuf[rows, :], w[...], preferred_element_type=F32).astype(BF16)
        qb[rows, :] = o[:, 0:128]
        kv[0, OWN + r0 : OWN + r0 + n, :] = o[:, 128:256]
        kv[1, OWN + r0 : OWN + r0 + n, :] = o[:, 256:384]

    phase("own_kv")
    for i in range(2):
        pl.semaphore_wait(far_sem.at[i], 1)

    def ctx_rows(ref, n, at):
        sq = jnp.zeros((n, 128), F32)
        for j in range(NT):
            v = ref[0 : n // CR, :, j * 128 : (j + 1) * 128].astype(F32).reshape(n, 128)
            sq += v * v
        cinv = lax.rsqrt(jnp.sum(sq, axis=1, keepdims=True) * (1.0 / D) + EPS)
        cinv = jnp.broadcast_to(cinv, (n, 128))
        for j in range(NT):
            cols = slice(j * 128, (j + 1) * 128)
            v = ref[0 : n // CR, :, cols].astype(F32).reshape(n, 128)
            hbuf[at : at + n, cols] = (v * cinv * mrow(1, j) + mrow(3, j)).astype(BF16)

    v_copies = [
        rcopy(
            kown, farin.at[FAR.index(ZN - d)], v_sem.at[0], v_sem.at[1], sp_z(d), t,
        )
        for d in far_order
    ]

    @pl.when(odd)
    def _():
        at = TOK + NB
        hbuf[at : at + 16, :] = jnp.zeros((16, D), BF16)
        ctx_rows(craw, CR, at)
        o = jnp.dot(hbuf[at : at + 16, :], w[:, 128:384], preferred_element_type=F32)
        for i in range(2):
            kown[i] = o[0:CR, i * 128 : (i + 1) * 128].astype(BF16)
        for cp in v_copies:
            cp.start()

    phase("proj_edge")
    project(TOK - BEFORE * GW, BEFORE * GW)
    to_next = rcopy(
        kv.at[:, KVN - (BEFORE + AFTER) * GW : KVN - AFTER * GW, :], kv.at[:, 0:OWN, :],
        h_sem.at[0], h_sem.at[1], s + 1, t,
    )

    @pl.when(has_next)
    def _():
        to_next.start()

    phase("fwd")
    fy_copies = [
        rcopy(yraw.at[i, :, half], yraw.at[i, :, half], fs_sem.at[i], fr_sem.at[i], s, tp_of(0, 1))
        for i in range(YH)
    ]
    f_copy = rcopy(
        craw.at[1:, :, half], craw.at[1:, :, half], f_sem.at[0], f_sem.at[1], s, tp_of(0, 1)
    )
    for i in range(YH):

        @pl.when(y != 2 * i)
        def _():
            arrived(yraw.at[i, :, half], ur_sem, i).wait_recv()
            fy_copies[i].start()

    @pl.when(odd)
    def _():
        z_all.wait_recv()
        f_copy.start()

    phase("proj_first")
    project(0, BEFORE * GW)
    to_prev = rcopy(
        kv.at[:, OWN : OWN + AFTER * GW, :], kv.at[:, KVN - AFTER * GW : KVN, :],
        h_sem.at[2], h_sem.at[3], s - 1, t,
    )

    @pl.when(has_prev)
    def _():
        to_prev.start()

    phase("ctx_z")
    @pl.when(even)
    def _():
        own_row.wait()

    for i in range(YH):

        @pl.when(y != 2 * i)
        def _():
            fy_copies[i].wait_recv()

    at = TOK + NB + 16
    ctx_rows(yraw, ZB, at)
    o = jnp.dot(hbuf[at : at + ZB, :], w[:, 128:384], preferred_element_type=F32)
    for i in range(2):
        kvz[0, i] = o[:, i * 128 : (i + 1) * 128].astype(BF16)
    k_copies = [
        rcopy(kvz.at[0], kvz.at[ZN - d], k_sem.at[0], k_sem.at[1], sp_z(d), t)
        for d in by_hops(range(1, ZN))
    ]
    for cp in k_copies:
        cp.start()

    phase("ctx_kv")
    y_copies = [
        rcopy(kvn.at[yi], kvn.at[yi], ys_sem.at[d], yr_sem.at[yi], sp_y(d), t) for d in y_order
    ]
    w_copies = [
        rcopy(kvf.at[yi], kvf.at[yi], ws_sem.at[d], wr_sem.at[yi], sp_y(d), t) for d in y_order
    ]

    @pl.when(odd)
    def _():
        f_copy.wait_recv()
        ctx_rows(craw, NB, TOK)
        o = jnp.dot(hbuf[TOK : TOK + NB, :], w[:, 128:384], preferred_element_type=F32)
        for i in range(2):
            kvn[yi, i] = o[:, i * 128 : (i + 1) * 128].astype(BF16)
        for cp in y_copies:
            cp.start()

    phase("proj_mid")
    project(BEFORE * GW, TOK - 2 * BEFORE * GW)

    factor = HD ** (-0.5)
    base = s * ROWS

    def window(r):
        g = base + r
        first_row = jnp.clip(g - WR // 2, 0, ALL_ROWS - WR)
        a0 = first_row - g + WR - 1
        k0 = pl.multiple_of((first_row - base + BEFORE) * GW, GW)
        rows = slice(r * GW, (r + 1) * GW)
        keys = kv[0, pl.ds(k0, WR * GW), :]
        vals = kv[1, pl.ds(k0, WR * GW), :]
        sc = lax.dot_general(qb[rows, :], keys, NT_DIMS, preferred_element_type=F32) * factor
        sc = jnp.concatenate(
            [sc[:, i * 128 : (i + 1) * 128] + bias[a0 + 2 * i] for i in range(WR // 2)], axis=1
        )
        m = jnp.max(sc, axis=1, keepdims=True)
        p = jnp.exp(sc - m)
        mwin[rows, :] = jnp.broadcast_to(m, (GW, 128))
        lwin[rows, :] = jnp.broadcast_to(jnp.sum(p, axis=1, keepdims=True), (GW, 128))
        owin[rows, :] = jnp.dot(p.astype(BF16), vals, preferred_element_type=F32)

    phase("win_mid")
    for r in range(BEFORE, ROWS - AFTER):
        window(r)

    phase("await_far")

    @pl.when(odd)
    def _():
        v_all.wait_recv()
        for i in range(2):
            kvf[yi, i] = farin[:, i].astype(F32).reshape(FB, HD).astype(BF16)
        for cp in w_copies:
            cp.start()

    phase("await_halo")

    @pl.when(has_prev)
    def _():
        to_next.wait_recv()

    @pl.when(has_next)
    def _():
        to_prev.wait_recv()

    phase("win_edge")
    for r in (*range(BEFORE), *range(ROWS - AFTER, ROWS)):
        window(r)

    def merge(rows, parts):
        q = qb[rows, :]
        scs = []
        for ctx in parts:
            keys = ctx[:, 0].reshape(-1, HD)
            sc = lax.dot_general(q, keys, NT_DIMS, preferred_element_type=F32) * factor
            scs.append(sc)
        m0 = mwin[rows, :]
        m = m0
        for sc in scs:
            m = jnp.maximum(m, jnp.max(sc, axis=1, keepdims=True))
        alpha = jnp.exp(m0 - m)
        den = alpha * lwin[rows, :]
        o = alpha * owin[rows, :]
        for ctx, sc in zip(parts, scs):
            vals = ctx[:, 1].reshape(-1, HD)
            p = jnp.concatenate(
                [jnp.exp(sc[:, i * 128 : (i + 1) * 128] - m) for i in range(sc.shape[1] // 128)],
                axis=1,
            )
            den += jnp.sum(p, axis=1, keepdims=True)
            o += jnp.dot(p.astype(BF16), vals, preferred_element_type=F32)
        return m, den, o

    phase("await_y")
    for i in range(YH):

        @pl.when(y != 2 * i + 1)
        def _():
            arrived(kvn.at[i], yr_sem, i).wait_recv()

    phase("ctx_near")
    for b in range(4):
        rows = slice(b * 160, (b + 1) * 160)
        mwin[rows, :], lwin[rows, :], owin[rows, :] = merge(rows, (kvn,))
    phase("await_k")
    for i in range(YH):

        @pl.when(y != 2 * i + 1)
        def _():
            arrived(kvf.at[i], wr_sem, i).wait_recv()

    phase("await_k2")
    k_all.wait_recv()
    phase("ctx_attn")
    for pair in ((2, 1), (3, 0)):
        done = []
        for dx in pair:
            chip = lax.rem(x + dx, XN)
            _, den, o = merge(pl.ds(pl.multiple_of(chip * 160, 160), 160), (kvf, kvz))
            done.append((o / den).astype(BF16))
        for dx, o in zip(pair, done):
            attn[2 * dx] = o[0:80]
            attn[2 * dx + 1] = o[80:160]
        for dx in pair:
            chip = lax.rem(x + dx, XN)
            if dx == 0:
                rcopy(attn.at[1 - c], own.at[c], o_sem.at[0], or_sem.at[0], s, tp_of(0, 1)).start()
                own[c] = attn[c]
                continue
            for cc in range(2):
                rcopy(
                    attn.at[2 * dx + cc], own.at[2 * dx + c], o_sem.at[0], or_sem.at[dx],
                    s, chip * 2 + cc,
                ).start()

    phase("out_proj")
    with jax.named_scope("await_g"):
        g_all.wait_recv()
    for f in range(2):
        hh = c if f == 0 else 1 - c
        mod[hh, 4] = redg[f] + redg[2 + f] + redg[4 + f] + redg[6 + f]
    loads["ow"].wait()
    for n, dx in enumerate((0, 1, 3, 2)):
        got = own.at[1 - c] if dx == 0 else own.at[2 * dx : 2 * dx + 2]
        rcopy(got, got, o_sem.at[0], or_sem.at[dx], s, tp_of(0, 1)).wait_recv()
        lhs = jnp.concatenate([own[2 * dx], own[2 * dx + 1]], axis=1)
        chip = lax.rem(x + XN - dx, XN)
        wrows = pl.ds(pl.multiple_of(chip * 256, 256), 256)
        res = pl.ds(pl.multiple_of(t * 80, 80), 80)
        for q in range(8):
            cols = slice(q * 256, (q + 1) * 256)
            o = jnp.dot(lhs, wo[wrows, cols], preferred_element_type=F32)
            if n > 0:
                o += acc[:, cols]
            if n < 3:
                acc[:, cols] = o
            else:
                for i in range(2):
                    j = 2 * q + i
                    jc = slice(j * 128, (j + 1) * 128)
                    v = lat[res, jc].astype(F32) + mrow(4, j) * o[:, i * 128 : (i + 1) * 128]
                    out_ref[:, jc] = v.astype(BF16)

    phase("drain")
    for cp in (a_copy, g_copy, b_all, g_all, k_all, o_all):
        cp.wait_send()

    @pl.when(odd)
    def _():
        for cp in (f_copy, z_all, v_all, *y_copies, *w_copies):
            cp.wait_send()

    @pl.when(even)
    def _():
        u_all.wait_send()

    for i in range(YH):

        @pl.when(y != 2 * i)
        def _():
            fy_copies[i].wait_send()

    @pl.when(has_next)
    def _():
        to_next.wait_send()

    @pl.when(has_prev)
    def _():
        to_prev.wait_send()

    phase(None)


def shards(
    latents, cond, ctx_cond, context, norm_gain, shift_weight, scale_weight, gate_weight,
    q_weight, k_weight, v_weight, out_weight, rel_bias,
):
    dma = pltpu.SemaphoreType.DMA
    scratch = [
        pltpu.VMEM((TOK, D), BF16),
        pltpu.VMEM((NT, 128), F32),
        pltpu.VMEM((NT, 128), F32),
        pltpu.VMEM((len(NEAR), CR, D), BF16),
        pltpu.VMEM((NT, 128), F32),
        pltpu.VMEM((3, 256, D), BF16),
        pltpu.VMEM((D, 384), BF16),
        pltpu.VMEM((1024, D), BF16),
        pltpu.VMEM((15, 1, 31), F32),
        pltpu.VMEM((2, 5, 8, 128), F32),
        pltpu.VMEM((5, 8, 128), F32),
        pltpu.VMEM((2 * XN, 4, 8, 128), BF16),
        pltpu.VMEM((2 * XN, 8, 128), F32),
        pltpu.VMEM((2, 5, 8, 128), F32),
        pltpu.VMEM((TOK, 128), F32),
        pltpu.VMEM((14, GW, 128), F32),
        pltpu.VMEM((TOK + NB + 16 + ZB, D), BF16),
        pltpu.VMEM((TOK, HD), BF16),
        pltpu.VMEM((2, KVN, HD), BF16),
        pltpu.VMEM((2, CR, HD), BF16),
        pltpu.VMEM((len(FAR), 2, CR, HD), BF16),
        pltpu.VMEM((YH, 2, NB, HD), BF16),
        pltpu.VMEM((YH, 2, FB, HD), BF16),
        pltpu.VMEM((ZN, 2, ZB, HD), BF16),
        pltpu.VMEM((YH, CR, D), BF16),
        pltpu.VMEM((TOK, HD), F32),
        pltpu.VMEM((TOK, HD), F32),
        pltpu.VMEM((TOK, HD), F32),
        pltpu.VMEM((8, 80, HD), BF16),
        pltpu.VMEM((8, 80, HD), BF16),
        pltpu.VMEM((80, D), F32),
        dma((14,)), dma((4,)), dma((4,)), dma((2,)), dma((2,)), dma((YN,)), dma((YH,)), dma((YN,)),
        dma((YH,)), dma((2,)), pltpu.SemaphoreType.REGULAR((2,)), dma((2,)), dma((YH,)), dma((YH,)),
        dma((YH,)), dma((2,)), dma((4,)), dma((2,)), dma((XN,)),
    ]
    anyspec = pl.BlockSpec(memory_space=pl.ANY)
    operands = (
        latents, cond.reshape(NT, 128), ctx_cond.reshape(NT, 128), context, norm_gain.reshape(NT, 128),
        shift_weight, scale_weight, gate_weight, q_weight, k_weight, v_weight, out_weight,
        rel_bias.transpose(1, 0, 2),
    )
    return pl.pallas_call(
        body,
        out_shape=jax.ShapeDtypeStruct((80, D), BF16),
        in_specs=[anyspec] * len(operands),
        out_specs=pl.BlockSpec(memory_space=pltpu.VMEM),
        scratch_shapes=scratch,
        compiler_params=pltpu.CompilerParams(
            collective_id=0, has_side_effects=True, vmem_limit_bytes=40 * 1024 * 1024
        ),
        name="step",
    )(*(pltpu.with_memory_space_constraint(v, pltpu.HBM) for v in operands))


def solution(mesh):
    in_specs = (
        P("sp", None),
        P(),
        P(),
        P("sp", None),
        P(),
        P("tp", None),
        P("tp", None),
        P("tp", None),
        P(None, "tp"),
        P(None, "tp"),
        P(None, "tp"),
        P(),
        P("tp", None, None),
    )
    out_specs = P(("sp", "tp"), None)
    return jax.shard_map(shards, mesh=mesh, in_specs=in_specs, out_specs=out_specs, check_vma=False)
```

```python
import jax
import jax.numpy as jnp
from jax import lax
from jax.experimental import pallas as pl
from jax.experimental.pallas import tpu as pltpu
from jax.sharding import PartitionSpec as P

D = 2048
HD = 128
GW = 64
WR = 8
WC = 16
EPS = 1e-06
NEG = -1e30
ZN, YN, XN = 12, 8, 4
NT = D // 128
TOK = 640
ROWS = TOK // GW
ALL_ROWS = ROWS * ZN * YN
BEFORE, AFTER = 4, 3
OWN = BEFORE * GW
KVN = (BEFORE + ROWS + AFTER) * GW
CR = 8
NEAR = (0, 1, 2, 3, 4, 11, 10, 9)
FAR = (5, 6, 7, 8)
NB, FB = CR * len(NEAR), CR * len(FAR)
YH = YN // 2
ZB = CR * YH
F32 = jnp.float32
BF16 = jnp.bfloat16
NT_DIMS = (((1,), (1,)), ((), ()))


def body(
    lat_h, cond_h, cctx_h, ctx_h, gain_h, shw_h, scw_h, gtw_h, qw_h, kw_h, vw_h, ow_h, rb_h,
    out_ref,
    lat, cond, craw, gain, mw, w, wo, rb,
    part, recva, red, redg, mod, inv, bias, hbuf, qb, kv, kown, farin, kvn, kvf, kvz, yraw,
    mwin, lwin, owin, attn, own, acc,
    in_sem, a_sem, b_sem, z_sem, f_sem, y_sem, yr_sem, wr_sem, v_sem, far_sem, u_sem, ur_sem,
    fs_sem, fr_sem, k_sem, h_sem, o_sem, or_sem,
):
    s = lax.axis_index("sp")
    t = lax.axis_index("tp")
    z, y = s // YN, s % YN
    x, c = t // 2, t % 2
    yi = y // 2
    even, odd = y % 2 == 0, y % 2 == 1

    def tp_of(dx, f):
        return lax.rem(x + dx, XN) * 2 + (c if f == 0 else 1 - c)

    tp_peers = [(dx, f) for dx in (2, 1, 3, 0) for f in (0, 1) if (dx, f) != (0, 0)]
    def by_hops(offsets):
        return sorted(offsets, key=lambda d: -min(d, ZN - d))

    raw_order = by_hops((-o) % ZN for o in NEAR[1:])
    far_order = by_hops((-o) % ZN for o in FAR)
    meet_order = by_hops((1, 2, 3, 4, 8, 9, 10, 11))
    y_order = sorted(range(1, YN), key=lambda d: -min(d, YN - d))

    scope = []

    def phase(name):
        while scope:
            scope.pop().__exit__(None, None, None)
        if name:
            scope.append(jax.named_scope(name))
            scope[0].__enter__()

    phase("hello")
    barrier = pltpu.get_barrier_semaphore()

    def hello(sp, tp):
        pl.semaphore_signal(
            barrier, inc=1, device_id={"sp": sp, "tp": tp}, device_id_type=pl.DeviceIdType.MESH
        )

    def sp_z(d):
        return lax.rem(z + d, ZN) * YN + y

    def sp_y(d):
        return z * YN + lax.rem(y + d, YN)

    for d in meet_order:
        hello(sp_z(d), t)
    for d in y_order:
        hello(sp_y(d), t)
    for dx, f in tp_peers:
        hello(s, tp_of(dx, f))
    has_next = s < ZN * YN - 1
    has_prev = s > 0
    next_far = jnp.logical_and(y == YN - 1, has_next)
    prev_far = jnp.logical_and(y == 0, has_prev)

    @pl.when(next_far)
    def _():
        hello(s + 1, t)

    @pl.when(prev_far)
    def _():
        hello(s - 1, t)

    loads = {}

    def load(name, k, src, dst):
        loads[name] = pltpu.make_async_copy(src, dst, in_sem.at[k])
        loads[name].start()

    load("ctx", 5, ctx_h, craw.at[0])
    own_row = pltpu.make_async_copy(ctx_h, yraw.at[yi], in_sem.at[1])

    @pl.when(even)
    def _():
        own_row.start()

    load("cond", 0, cond_h, cond.at[0])
    load("cctx", 0, cctx_h, cond.at[1])
    load("sc", 2, scw_h, mw.at[0])
    load("sh", 3, shw_h, mw.at[1])
    load("rb", 6, rb_h, rb)
    load("gain", 7, gain_h, gain)
    load("gt", 4, gtw_h, mw.at[2])
    load("lat", 8, lat_h, lat)
    load("qw", 9, qw_h, w.at[:, 0:128])
    load("kw", 9, kw_h, w.at[:, 128:256])
    load("vw", 9, vw_h, w.at[:, 256:384])
    load("ow", 10, ow_h, wo)

    def rcopy(src, dst, ssem, rsem, sp, tp):
        return pltpu.make_async_remote_copy(
            src_ref=src, dst_ref=dst, send_sem=ssem, recv_sem=rsem,
            device_id={"sp": sp, "tp": tp}, device_id_type=pl.DeviceIdType.MESH,
        )

    def silu_row(ref):
        v = jnp.concatenate([ref[pl.ds(2 * t, 1), :], ref[pl.ds(2 * t + 1, 1), :]], axis=1)
        return (v / (1.0 + jnp.exp(-v))).astype(BF16)

    half = pl.ds(pl.multiple_of(c * 1024, 1024), 1024)
    z_copies = [
        rcopy(
            craw.at[0, :, half], craw.at[NEAR.index(ZN - d), :, half], z_sem.at[0], z_sem.at[1],
            sp_z(d), t,
        )
        for d in raw_order
    ]

    y_raw = [
        rcopy(craw.at[0, :, half], yraw.at[yi, :, half], u_sem.at[0], ur_sem.at[yi], sp_y(d), t)
        for d in y_order
    ]

    def arrived(ref, sem, i):
        return rcopy(ref, ref, u_sem.at[0], sem.at[i], sp_y(1), t)

    def meet():
        with jax.named_scope("meet"):
            loads["ctx"].wait()
            pl.semaphore_wait(
                barrier,
                len(meet_order) + YN - 1 + 2 * XN - 1 + next_far.astype(jnp.int32) + prev_far.astype(jnp.int32),
            )

            @pl.when(odd)
            def _():
                for cp in z_copies:
                    cp.start()

            @pl.when(even)
            def _():
                for cp in y_raw:
                    cp.start()

            for i, d in enumerate((3, ZN - 3)):
                pl.semaphore_signal(
                    far_sem.at[i], inc=1, device_id={"sp": sp_z(d), "tp": t},
                    device_id_type=pl.DeviceIdType.MESH,
                )

    late = jnp.logical_and(z >= 7, y >= 4)

    @pl.when(late)
    def _():
        meet()

    def act_rows():
        row = lax.broadcasted_iota(jnp.int32, (16, 256), 0)
        return jnp.where(
            row == 0,
            silu_row(cond.at[0]).astype(F32),
            jnp.where(row == 1, silu_row(cond.at[1]).astype(F32), 0.0),
        ).astype(BF16)

    def partial(k, name):
        act = act_rows()
        loads[name].wait()
        for n in range(8):
            o = jnp.dot(act, mw[k, :, n * 256 : (n + 1) * 256], preferred_element_type=F32)
            for i in range(2):
                j = 2 * n + i
                piece = o[:, i * 128 : (i + 1) * 128]
                for r in range(1 if k == 2 else 2):
                    part[j // 8, 2 * k + r, j % 8 : j % 8 + 1, :] = piece[r : r + 1, :]

    with jax.named_scope("partials"):
        pltpu.make_async_copy(cond, cond, in_sem.at[0]).wait()
        partial(0, "sc")
        partial(1, "sh")

    @pl.when(jnp.logical_not(late))
    def _():
        meet()

    vec, gate = slice(0, 4), slice(4, 5)
    a_copy = rcopy(part.at[1 - c, vec], recva.at[vec], a_sem.at[0], a_sem.at[1], s, tp_of(0, 1))
    g_copy = rcopy(part.at[1 - c, gate], recva.at[gate], a_sem.at[2], a_sem.at[3], s, tp_of(0, 1))
    a_copy.start()
    with jax.named_scope("gatepart"):
        partial(2, "gt")
    g_copy.start()
    with jax.named_scope("await_a"):
        a_copy.wait_recv()
    red[0] = (part[c, vec] + recva[vec]).astype(BF16)
    b_copies = [
        rcopy(
            red.at[0], red.at[2 * dx + f], b_sem.at[0], b_sem.at[1], s, tp_of(dx, f),
        )
        for dx, f in tp_peers
    ]
    g_copies = [
        rcopy(
            redg.at[0], redg.at[2 * dx + f], b_sem.at[2], b_sem.at[3], s, tp_of(dx, f),
        )
        for dx, f in tp_peers
    ]
    for cp in b_copies:
        cp.start()

    def together(ref, sems):
        return rcopy(ref, ref, sems.at[0], sems.at[1], s, tp_of(0, 1))

    b_all = together(red.at[1:], b_sem.at[0:2])
    g_all = together(redg.at[1:], b_sem.at[2:4])
    z_all = together(craw.at[1:, :, half], z_sem)
    u_all = together(craw.at[1:, :, half], u_sem)
    v_all = together(farin, v_sem)
    k_all = together(kvz.at[1:], k_sem)
    o_all = together(attn.at[1:], o_sem)
    y_all = together(kvn.at[1:], y_sem)
    w_all = rcopy(kvf.at[1:], kvf.at[1:], y_sem.at[1], y_sem.at[0], s, tp_of(0, 1))

    phase("bias")
    loads["rb"].wait()
    rb_rows = [jnp.concatenate([rb[a], jnp.zeros((1, 97), F32)], axis=1) for a in range(15)]
    lane = lax.broadcasted_iota(jnp.int32, (1, 128), 1)
    qcol = lax.broadcasted_iota(jnp.int32, (GW, 128), 0)
    kcol = lax.broadcasted_iota(jnp.int32, (GW, 128), 1) % GW
    first = jnp.clip(qcol - WC // 2, 0, GW - WC)
    inside = jnp.logical_and(kcol >= first, kcol < first + WC)
    for a in range(14):
        v = jnp.where(
            jnp.logical_and(lane >= 49, lane <= 79),
            pltpu.roll(rb_rows[a + 1], 49, 1),
            pltpu.roll(rb_rows[a], 113, 1),
        )
        spread = pltpu.roll(jnp.broadcast_to(v, (GW, 128)), 0, 1, stride=1, stride_axis=0)
        bias[a] = jnp.where(inside, spread, NEG)

    phase("rms")
    loads["lat"].wait()
    for b in range(TOK // 128):
        rows = slice(b * 128, (b + 1) * 128)
        sq = jnp.zeros((128, 128), F32)
        for j in range(NT):
            v = lat[rows, j * 128 : (j + 1) * 128].astype(F32)
            sq += v * v
        mean = jnp.sum(sq, axis=1, keepdims=True) * (1.0 / D)
        inv[rows, :] = jnp.broadcast_to(lax.rsqrt(mean + EPS), (128, 128))

    phase("send_g")
    g_copy.wait_recv()
    redg[0] = part[c, 4] + recva[4]
    for cp in g_copies:
        cp.start()
    with jax.named_scope("await_b"):
        b_all.wait_recv()
    loads["gain"].wait()
    for f in range(2):
        tot = sum(red[2 * k + f].astype(F32) for k in range(XN))
        hh = c if f == 0 else 1 - c
        gn = gain[pl.ds(pl.multiple_of(hh * 8, 8), 8), :]
        mod[hh, 0] = gn * (1.0 + tot[0])
        mod[hh, 1] = gn * (1.0 + tot[1])
        mod[hh, 2] = tot[2]
        mod[hh, 3] = tot[3]

    def mrow(v, j):
        return mod[j // 8, v, j % 8 : j % 8 + 1, :]

    pltpu.make_async_copy(w, w, in_sem.at[9]).wait()

    def project(r0, n):
        rows = slice(r0, r0 + n)
        for j in range(NT):
            cols = slice(j * 128, (j + 1) * 128)
            v = lat[rows, cols].astype(F32) * inv[rows, :] * mrow(0, j) + mrow(2, j)
            hbuf[rows, cols] = v.astype(BF16)
        o = jnp.dot(hbuf[rows, :], w[...], preferred_element_type=F32).astype(BF16)
        qb[rows, :] = o[:, 0:128]
        kv[0, OWN + r0 : OWN + r0 + n, :] = o[:, 128:256]
        kv[1, OWN + r0 : OWN + r0 + n, :] = o[:, 256:384]

    phase("own_kv")
    for i in range(2):
        pl.semaphore_wait(far_sem.at[i], 1)

    def ctx_rows(ref, n, at):
        sq = jnp.zeros((n, 128), F32)
        for j in range(NT):
            v = ref[0 : n // CR, :, j * 128 : (j + 1) * 128].astype(F32).reshape(n, 128)
            sq += v * v
        cinv = lax.rsqrt(jnp.sum(sq, axis=1, keepdims=True) * (1.0 / D) + EPS)
        cinv = jnp.broadcast_to(cinv, (n, 128))
        for j in range(NT):
            cols = slice(j * 128, (j + 1) * 128)
            v = ref[0 : n // CR, :, cols].astype(F32).reshape(n, 128)
            hbuf[at : at + n, cols] = (v * cinv * mrow(1, j) + mrow(3, j)).astype(BF16)

    v_copies = [
        rcopy(
            kown, farin.at[FAR.index(ZN - d)], v_sem.at[0], v_sem.at[1], sp_z(d), t,
        )
        for d in far_order
    ]

    @pl.when(odd)
    def _():
        at = TOK + NB
        hbuf[at : at + 16, :] = jnp.zeros((16, D), BF16)
        ctx_rows(craw, CR, at)
        o = jnp.dot(hbuf[at : at + 16, :], w[:, 128:384], preferred_element_type=F32)
        for i in range(2):
            kown[i] = o[0:CR, i * 128 : (i + 1) * 128].astype(BF16)
        for cp in v_copies:
            cp.start()

    phase("proj_edge")
    project(TOK - BEFORE * GW, BEFORE * GW)
    to_next = rcopy(
        kv.at[:, KVN - (BEFORE + AFTER) * GW : KVN - AFTER * GW, :], kv.at[:, 0:OWN, :],
        h_sem.at[0], h_sem.at[1], s + 1, t,
    )

    @pl.when(has_next)
    def _():
        to_next.start()

    phase("fwd")
    fy_copies = [
        rcopy(yraw.at[i, :, half], yraw.at[i, :, half], fs_sem.at[i], fr_sem.at[i], s, tp_of(0, 1))
        for i in range(YH)
    ]
    f_copy = rcopy(
        craw.at[1:, :, half], craw.at[1:, :, half], f_sem.at[0], f_sem.at[1], s, tp_of(0, 1)
    )
    for i in range(YH):

        @pl.when(y != 2 * i)
        def _():
            arrived(yraw.at[i, :, half], ur_sem, i).wait_recv()
            fy_copies[i].start()

    @pl.when(odd)
    def _():
        z_all.wait_recv()
        f_copy.start()

    phase("proj_first")
    project(0, BEFORE * GW)
    to_prev = rcopy(
        kv.at[:, OWN : OWN + AFTER * GW, :], kv.at[:, KVN - AFTER * GW : KVN, :],
        h_sem.at[2], h_sem.at[3], s - 1, t,
    )

    @pl.when(has_prev)
    def _():
        to_prev.start()

    phase("ctx_z")
    @pl.when(even)
    def _():
        own_row.wait()

    for i in range(YH):

        @pl.when(y != 2 * i)
        def _():
            fy_copies[i].wait_recv()

    at = TOK + NB + 16
    ctx_rows(yraw, ZB, at)
    o = jnp.dot(hbuf[at : at + ZB, :], w[:, 128:384], preferred_element_type=F32)
    for i in range(2):
        kvz[0, i] = o[:, i * 128 : (i + 1) * 128].astype(BF16)
    k_copies = [
        rcopy(kvz.at[0], kvz.at[ZN - d], k_sem.at[0], k_sem.at[1], sp_z(d), t)
        for d in by_hops(range(1, ZN))
    ]
    for cp in k_copies:
        cp.start()

    phase("ctx_kv")
    y_copies = [
        rcopy(kvn.at[yi], kvn.at[yi], y_sem.at[0], yr_sem.at[yi], sp_y(d), t) for d in y_order
    ]
    w_copies = [
        rcopy(kvf.at[yi], kvf.at[yi], y_sem.at[1], wr_sem.at[yi], sp_y(d), t) for d in y_order
    ]

    @pl.when(odd)
    def _():
        f_copy.wait_recv()
        ctx_rows(craw, NB, TOK)
        o = jnp.dot(hbuf[TOK : TOK + NB, :], w[:, 128:384], preferred_element_type=F32)
        for i in range(2):
            kvn[yi, i] = o[:, i * 128 : (i + 1) * 128].astype(BF16)
        for cp in y_copies:
            cp.start()

    phase("proj_mid")
    project(BEFORE * GW, TOK - 2 * BEFORE * GW)

    factor = HD ** (-0.5)
    base = s * ROWS

    def window(r):
        g = base + r
        first_row = jnp.clip(g - WR // 2, 0, ALL_ROWS - WR)
        a0 = first_row - g + WR - 1
        k0 = pl.multiple_of((first_row - base + BEFORE) * GW, GW)
        rows = slice(r * GW, (r + 1) * GW)
        keys = kv[0, pl.ds(k0, WR * GW), :]
        vals = kv[1, pl.ds(k0, WR * GW), :]
        sc = lax.dot_general(qb[rows, :], keys, NT_DIMS, preferred_element_type=F32) * factor
        sc = jnp.concatenate(
            [sc[:, i * 128 : (i + 1) * 128] + bias[a0 + 2 * i] for i in range(WR // 2)], axis=1
        )
        m = jnp.max(sc, axis=1, keepdims=True)
        p = jnp.exp(sc - m)
        mwin[rows, :] = jnp.broadcast_to(m, (GW, 128))
        lwin[rows, :] = jnp.broadcast_to(jnp.sum(p, axis=1, keepdims=True), (GW, 128))
        owin[rows, :] = jnp.dot(p.astype(BF16), vals, preferred_element_type=F32)

    phase("win_mid")
    for r in range(BEFORE, ROWS - AFTER):
        window(r)

    phase("await_far")

    @pl.when(odd)
    def _():
        v_all.wait_recv()
        for i in range(2):
            kvf[yi, i] = farin[:, i].astype(F32).reshape(FB, HD).astype(BF16)
        for cp in w_copies:
            cp.start()

    phase("await_halo")

    @pl.when(has_prev)
    def _():
        to_next.wait_recv()

    @pl.when(has_next)
    def _():
        to_prev.wait_recv()

    phase("win_edge")
    for r in (*range(BEFORE), *range(ROWS - AFTER, ROWS)):
        window(r)

    def merge(rows, parts):
        q = qb[rows, :]
        scs = []
        for ctx in parts:
            keys = ctx[:, 0].reshape(-1, HD)
            sc = lax.dot_general(q, keys, NT_DIMS, preferred_element_type=F32) * factor
            scs.append(sc)
        m0 = mwin[rows, :]
        m = m0
        for sc in scs:
            m = jnp.maximum(m, jnp.max(sc, axis=1, keepdims=True))
        alpha = jnp.exp(m0 - m)
        den = alpha * lwin[rows, :]
        o = alpha * owin[rows, :]
        for ctx, sc in zip(parts, scs):
            vals = ctx[:, 1].reshape(-1, HD)
            p = jnp.concatenate(
                [jnp.exp(sc[:, i * 128 : (i + 1) * 128] - m) for i in range(sc.shape[1] // 128)],
                axis=1,
            )
            den += jnp.sum(p, axis=1, keepdims=True)
            o += jnp.dot(p.astype(BF16), vals, preferred_element_type=F32)
        return m, den, o

    phase("await_y")
    for i in range(YH):

        @pl.when(y != 2 * i + 1)
        def _():
            arrived(kvn.at[i], yr_sem, i).wait_recv()

    phase("ctx_near")
    for b in range(4):
        rows = slice(b * 160, (b + 1) * 160)
        mwin[rows, :], lwin[rows, :], owin[rows, :] = merge(rows, (kvn.at[0:YH],))
    phase("await_k")
    for i in range(YH):

        @pl.when(y != 2 * i + 1)
        def _():
            arrived(kvf.at[i], wr_sem, i).wait_recv()

    phase("await_k2")
    k_all.wait_recv()
    phase("ctx_attn")
    for pair in ((2, 1), (3,), (0,)):
        done = []
        for dx in pair:
            chip = lax.rem(x + dx, XN)
            _, den, o = merge(pl.ds(pl.multiple_of(chip * 160, 160), 160), (kvf.at[0:YH], kvz))
            done.append((o / den).astype(BF16))
        for dx, o in zip(pair, done):
            attn[2 * dx] = o[0:80]
            attn[2 * dx + 1] = o[80:160]
        for dx in pair:
            chip = lax.rem(x + dx, XN)
            if dx == 0:
                rcopy(attn.at[1 - c], own.at[c], o_sem.at[0], or_sem.at[0], s, tp_of(0, 1)).start()
                own[c] = attn[c]
                continue
            for cc in range(2):
                rcopy(
                    attn.at[2 * dx + cc], own.at[2 * dx + c], o_sem.at[0], or_sem.at[dx],
                    s, chip * 2 + cc,
                ).start()

    phase("out_proj")
    with jax.named_scope("await_g"):
        g_all.wait_recv()
    for f in range(2):
        hh = c if f == 0 else 1 - c
        mod[hh, 4] = redg[f] + redg[2 + f] + redg[4 + f] + redg[6 + f]
    loads["ow"].wait()
    for n, dx in enumerate((0, 1, 3, 2)):
        got = own.at[1 - c] if dx == 0 else own.at[2 * dx : 2 * dx + 2]
        rcopy(got, got, o_sem.at[0], or_sem.at[dx], s, tp_of(0, 1)).wait_recv()
        lhs = jnp.concatenate([own[2 * dx], own[2 * dx + 1]], axis=1)
        chip = lax.rem(x + XN - dx, XN)
        wrows = pl.ds(pl.multiple_of(chip * 256, 256), 256)
        res = pl.ds(pl.multiple_of(t * 80, 80), 80)
        for q in range(8):
            cols = slice(q * 256, (q + 1) * 256)
            o = jnp.dot(lhs, wo[wrows, cols], preferred_element_type=F32)
            if n > 0:
                o += acc[:, cols]
            if n < 3:
                acc[:, cols] = o
            else:
                for i in range(2):
                    j = 2 * q + i
                    jc = slice(j * 128, (j + 1) * 128)
                    v = lat[res, jc].astype(F32) + mrow(4, j) * o[:, i * 128 : (i + 1) * 128]
                    out_ref[:, jc] = v.astype(BF16)

    phase("drain")
    for cp in (a_copy, g_copy, b_all, g_all, k_all, o_all):
        cp.wait_send()

    @pl.when(odd)
    def _():
        for cp in (f_copy, z_all, v_all, y_all, w_all):
            cp.wait_send()

    @pl.when(even)
    def _():
        u_all.wait_send()

    for i in range(YH):

        @pl.when(y != 2 * i)
        def _():
            fy_copies[i].wait_send()

    @pl.when(has_next)
    def _():
        to_next.wait_send()

    @pl.when(has_prev)
    def _():
        to_prev.wait_send()

    phase(None)


def shards(
    latents, cond, ctx_cond, context, norm_gain, shift_weight, scale_weight, gate_weight,
    q_weight, k_weight, v_weight, out_weight, rel_bias,
):
    dma = pltpu.SemaphoreType.DMA
    scratch = [
        pltpu.VMEM((TOK, D), BF16),
        pltpu.VMEM((2, NT, 128), F32),
        pltpu.VMEM((len(NEAR), CR, D), BF16),
        pltpu.VMEM((NT, 128), F32),
        pltpu.VMEM((3, 256, D), BF16),
        pltpu.VMEM((D, 384), BF16),
        pltpu.VMEM((1024, D), BF16),
        pltpu.VMEM((15, 1, 31), F32),
        pltpu.VMEM((2, 5, 8, 128), F32),
        pltpu.VMEM((5, 8, 128), F32),
        pltpu.VMEM((2 * XN, 4, 8, 128), BF16),
        pltpu.VMEM((2 * XN, 8, 128), F32),
        pltpu.VMEM((2, 5, 8, 128), F32),
        pltpu.VMEM((TOK, 128), F32),
        pltpu.VMEM((14, GW, 128), F32),
        pltpu.VMEM((TOK + NB + 16 + ZB, D), BF16),
        pltpu.VMEM((TOK, HD), BF16),
        pltpu.VMEM((2, KVN, HD), BF16),
        pltpu.VMEM((2, CR, HD), BF16),
        pltpu.VMEM((len(FAR), 2, CR, HD), BF16),
        pltpu.VMEM((YN, 2, NB, HD), BF16),
        pltpu.VMEM((YN, 2, FB, HD), BF16),
        pltpu.VMEM((ZN, 2, ZB, HD), BF16),
        pltpu.VMEM((YH, CR, D), BF16),
        pltpu.VMEM((TOK, HD), F32),
        pltpu.VMEM((TOK, HD), F32),
        pltpu.VMEM((TOK, HD), F32),
        pltpu.VMEM((8, 80, HD), BF16),
        pltpu.VMEM((8, 80, HD), BF16),
        pltpu.VMEM((80, D), F32),
        dma((11,)), dma((4,)), dma((4,)), dma((2,)), dma((2,)), dma((2,)), dma((YH,)),
        dma((YH,)), dma((2,)), pltpu.SemaphoreType.REGULAR((2,)), dma((2,)), dma((YH,)), dma((YH,)),
        dma((YH,)), dma((2,)), dma((4,)), dma((2,)), dma((XN,)),
    ]
    anyspec = pl.BlockSpec(memory_space=pl.ANY)
    operands = (
        latents, cond.reshape(NT, 128), ctx_cond.reshape(NT, 128), context, norm_gain.reshape(NT, 128),
        shift_weight, scale_weight, gate_weight, q_weight, k_weight, v_weight, out_weight,
        rel_bias.transpose(1, 0, 2),
    )
    return pl.pallas_call(
        body,
        out_shape=jax.ShapeDtypeStruct((80, D), BF16),
        in_specs=[anyspec] * len(operands),
        out_specs=pl.BlockSpec(memory_space=pltpu.VMEM),
        scratch_shapes=scratch,
        compiler_params=pltpu.CompilerParams(
            collective_id=0, has_side_effects=True, vmem_limit_bytes=40 * 1024 * 1024
        ),
        name="step",
    )(*(pltpu.with_memory_space_constraint(v, pltpu.HBM) for v in operands))


def solution(mesh):
    in_specs = (
        P("sp", None),
        P(),
        P(),
        P("sp", None),
        P(),
        P("tp", None),
        P("tp", None),
        P("tp", None),
        P(None, "tp"),
        P(None, "tp"),
        P(None, "tp"),
        P(),
        P("tp", None, None),
    )
    out_specs = P(("sp", "tp"), None)
    return jax.shard_map(shards, mesh=mesh, in_specs=in_specs, out_specs=out_specs, check_vma=False)
```

```python
import functools

import jax
import jax.numpy as jnp
from jax import lax
from jax.experimental import pallas as pl
from jax.experimental.pallas import tpu as pltpu
from jax.sharding import PartitionSpec as P

D = 2048
HD = 128
GW = 64
WR = 8
WC = 16
EPS = 1e-06
NEG = -1e30
ZN, YN, XN = 12, 8, 4
NT = D // 128
TOK = 640
ROWS = TOK // GW
ALL_ROWS = ROWS * ZN * YN
BEFORE, AFTER = 4, 3
OWN = BEFORE * GW
KVN = (BEFORE + ROWS + AFTER) * GW
CR = 8
NEAR = (0, 1, 2, 3, 4, 11, 10, 9)
FAR = (5, 6, 7, 8)
NB, FB = CR * len(NEAR), CR * len(FAR)
YH = YN // 2
ZB = CR * YH
F32 = jnp.float32
BF16 = jnp.bfloat16
NT_DIMS = (((1,), (1,)), ((), ()))


def body(
    lat_h, cond_h, cctx_h, ctx_h, gain_h, shw_h, scw_h, gtw_h, qw_h, kw_h, vw_h, ow_h, rb_h,
    out_ref,
    lat, cond, craw, gain, mw, w, wo, rb,
    part, recva, red, redg, mod, inv, bias, hbuf, qb, kv, kown, farin, kvn, kvf, kvz, yraw,
    mwin, lwin, owin, attn, own, acc,
    in_sem, a_sem, b_sem, z_sem, f_sem, y_sem, yr_sem, wr_sem, v_sem, far_sem, u_sem, ur_sem,
    fs_sem, fr_sem, k_sem, h_sem, o_sem, or_sem,
):
    s = lax.axis_index("sp")
    t = lax.axis_index("tp")
    z, y = s // YN, s % YN
    x, c = t // 2, t % 2
    yi = y // 2
    even, odd = y % 2 == 0, y % 2 == 1

    def tp_of(dx, f):
        return lax.rem(x + dx, XN) * 2 + (c if f == 0 else 1 - c)

    tp_peers = [(dx, f) for dx in (2, 1, 3, 0) for f in (0, 1) if (dx, f) != (0, 0)]
    def by_hops(offsets):
        return sorted(offsets, key=lambda d: -min(d, ZN - d))

    raw_order = by_hops((-o) % ZN for o in NEAR[1:])
    far_order = by_hops((-o) % ZN for o in FAR)
    meet_order = by_hops((1, 2, 3, 4, 8, 9, 10, 11))
    y_order = sorted(range(1, YN), key=lambda d: -min(d, YN - d))

    scope = []

    def phase(name):
        while scope:
            scope.pop().__exit__(None, None, None)
        if name:
            scope.append(jax.named_scope(name))
            scope[0].__enter__()

    phase("hello")
    barrier = pltpu.get_barrier_semaphore()

    def hello(sp, tp):
        pl.semaphore_signal(
            barrier, inc=1, device_id={"sp": sp, "tp": tp}, device_id_type=pl.DeviceIdType.MESH
        )

    def sp_z(d):
        return lax.rem(z + d, ZN) * YN + y

    def sp_y(d):
        return z * YN + lax.rem(y + d, YN)

    for d in meet_order:
        hello(sp_z(d), t)
    for d in y_order:
        hello(sp_y(d), t)
    for dx, f in tp_peers:
        hello(s, tp_of(dx, f))
    has_next = s < ZN * YN - 1
    has_prev = s > 0
    next_far = jnp.logical_and(y == YN - 1, has_next)
    prev_far = jnp.logical_and(y == 0, has_prev)

    @pl.when(next_far)
    def _():
        hello(s + 1, t)

    @pl.when(prev_far)
    def _():
        hello(s - 1, t)

    loads = {}

    def load(name, k, src, dst):
        loads[name] = pltpu.make_async_copy(src, dst, in_sem.at[k])
        loads[name].start()

    load("ctx", 5, ctx_h, craw.at[0])
    own_row = pltpu.make_async_copy(ctx_h, yraw.at[yi], in_sem.at[1])

    @pl.when(even)
    def _():
        own_row.start()

    load("cond", 0, cond_h, cond.at[0])
    load("cctx", 0, cctx_h, cond.at[1])
    load("sc", 2, scw_h, mw.at[0])
    load("sh", 3, shw_h, mw.at[1])
    load("rb", 6, rb_h, rb)
    load("gain", 7, gain_h, gain)
    load("gt", 4, gtw_h, mw.at[2])
    load("lat", 8, lat_h, lat)
    load("qw", 9, qw_h, w.at[:, 0:128])
    load("kw", 9, kw_h, w.at[:, 128:256])
    load("vw", 9, vw_h, w.at[:, 256:384])
    load("ow", 10, ow_h, wo)

    def rcopy(src, dst, ssem, rsem, sp, tp):
        return pltpu.make_async_remote_copy(
            src_ref=src, dst_ref=dst, send_sem=ssem, recv_sem=rsem,
            device_id={"sp": sp, "tp": tp}, device_id_type=pl.DeviceIdType.MESH,
        )

    def silu_row(ref):
        v = jnp.concatenate([ref[pl.ds(2 * t, 1), :], ref[pl.ds(2 * t + 1, 1), :]], axis=1)
        return (v / (1.0 + jnp.exp(-v))).astype(BF16)

    half = pl.ds(pl.multiple_of(c * 1024, 1024), 1024)
    z_copies = [
        rcopy(
            craw.at[0, :, half], craw.at[NEAR.index(ZN - d), :, half], z_sem.at[0], z_sem.at[1],
            sp_z(d), t,
        )
        for d in raw_order
    ]

    y_raw = [
        rcopy(craw.at[0, :, half], yraw.at[yi, :, half], u_sem.at[0], ur_sem.at[yi], sp_y(d), t)
        for d in y_order
    ]

    def arrived(ref, sem, i):
        return rcopy(ref, ref, u_sem.at[0], sem.at[i], sp_y(1), t)

    def meet():
        with jax.named_scope("meet"):
            loads["ctx"].wait()
            pl.semaphore_wait(
                barrier,
                len(meet_order) + YN - 1 + 2 * XN - 1 + next_far.astype(jnp.int32) + prev_far.astype(jnp.int32),
            )

            @pl.when(odd)
            def _():
                for cp in z_copies:
                    cp.start()

            @pl.when(even)
            def _():
                for cp in y_raw:
                    cp.start()

            for i, d in enumerate((3, ZN - 3)):
                pl.semaphore_signal(
                    far_sem.at[i], inc=1, device_id={"sp": sp_z(d), "tp": t},
                    device_id_type=pl.DeviceIdType.MESH,
                )

    late = jnp.logical_and(z >= 7, y >= 4)

    @pl.when(late)
    def _():
        meet()

    def act_rows():
        row = lax.broadcasted_iota(jnp.int32, (16, 256), 0)
        return jnp.where(
            row == 0,
            silu_row(cond.at[0]).astype(F32),
            jnp.where(row == 1, silu_row(cond.at[1]).astype(F32), 0.0),
        ).astype(BF16)

    def partial(k, name):
        act = act_rows()
        loads[name].wait()
        for n in range(8):
            o = jnp.dot(act, mw[k, :, n * 256 : (n + 1) * 256], preferred_element_type=F32)
            for i in range(2):
                j = 2 * n + i
                piece = o[:, i * 128 : (i + 1) * 128]
                for r in range(1 if k == 2 else 2):
                    part[j // 8, 2 * k + r, j % 8 : j % 8 + 1, :] = piece[r : r + 1, :]

    with jax.named_scope("partials"):
        pltpu.make_async_copy(cond, cond, in_sem.at[0]).wait()
        partial(0, "sc")
        partial(1, "sh")

    @pl.when(jnp.logical_not(late))
    def _():
        meet()

    vec, gate = slice(0, 4), slice(4, 5)
    a_copy = rcopy(part.at[1 - c, vec], recva.at[vec], a_sem.at[0], a_sem.at[1], s, tp_of(0, 1))
    g_copy = rcopy(part.at[1 - c, gate], recva.at[gate], a_sem.at[2], a_sem.at[3], s, tp_of(0, 1))
    a_copy.start()
    with jax.named_scope("gatepart"):
        partial(2, "gt")
    g_copy.start()
    with jax.named_scope("await_a"):
        a_copy.wait_recv()
    red[0] = (part[c, vec] + recva[vec]).astype(BF16)
    b_copies = [
        rcopy(
            red.at[0], red.at[2 * dx + f], b_sem.at[0], b_sem.at[1], s, tp_of(dx, f),
        )
        for dx, f in tp_peers
    ]
    g_copies = [
        rcopy(
            redg.at[0], redg.at[2 * dx + f], b_sem.at[2], b_sem.at[3], s, tp_of(dx, f),
        )
        for dx, f in tp_peers
    ]
    for cp in b_copies:
        cp.start()

    def together(ref, sems):
        return rcopy(ref, ref, sems.at[0], sems.at[1], s, tp_of(0, 1))

    b_all = together(red.at[1:], b_sem.at[0:2])
    g_all = together(redg.at[1:], b_sem.at[2:4])
    z_all = together(craw.at[1:, :, half], z_sem)
    u_all = together(craw.at[1:, :, half], u_sem)
    v_all = together(farin, v_sem)
    k_all = together(kvz.at[1:], k_sem)
    o_all = together(attn.at[1:], o_sem)
    y_all = together(kvn.at[1:], y_sem)
    w_all = rcopy(kvf.at[1:], kvf.at[1:], y_sem.at[1], y_sem.at[0], s, tp_of(0, 1))

    phase("bias")
    loads["rb"].wait()
    rb_rows = [jnp.concatenate([rb[a], jnp.zeros((1, 97), F32)], axis=1) for a in range(15)]
    lane = lax.broadcasted_iota(jnp.int32, (1, 128), 1)
    qcol = lax.broadcasted_iota(jnp.int32, (GW, 128), 0)
    kcol = lax.broadcasted_iota(jnp.int32, (GW, 128), 1) % GW
    first = jnp.clip(qcol - WC // 2, 0, GW - WC)
    inside = jnp.logical_and(kcol >= first, kcol < first + WC)
    for a in range(14):
        v = jnp.where(
            jnp.logical_and(lane >= 49, lane <= 79),
            pltpu.roll(rb_rows[a + 1], 49, 1),
            pltpu.roll(rb_rows[a], 113, 1),
        )
        spread = pltpu.roll(jnp.broadcast_to(v, (GW, 128)), 0, 1, stride=1, stride_axis=0)
        bias[a] = jnp.where(inside, spread, NEG)

    phase("rms")
    loads["lat"].wait()
    for b in range(TOK // 128):
        rows = slice(b * 128, (b + 1) * 128)
        sq = jnp.zeros((128, 128), F32)
        for j in range(NT):
            v = lat[rows, j * 128 : (j + 1) * 128].astype(F32)
            sq += v * v
        mean = jnp.sum(sq, axis=1, keepdims=True) * (1.0 / D)
        inv[rows, :] = jnp.broadcast_to(lax.rsqrt(mean + EPS), (128, 128))

    phase("send_g")
    g_copy.wait_recv()
    redg[0] = part[c, 4] + recva[4]
    for cp in g_copies:
        cp.start()
    with jax.named_scope("await_b"):
        b_all.wait_recv()
    loads["gain"].wait()
    for f in range(2):
        tot = sum(red[2 * k + f].astype(F32) for k in range(XN))
        hh = c if f == 0 else 1 - c
        gn = gain[pl.ds(pl.multiple_of(hh * 8, 8), 8), :]
        mod[hh, 0] = gn * (1.0 + tot[0])
        mod[hh, 1] = gn * (1.0 + tot[1])
        mod[hh, 2] = tot[2]
        mod[hh, 3] = tot[3]

    def mrow(v, j):
        return mod[j // 8, v, j % 8 : j % 8 + 1, :]

    pltpu.make_async_copy(w, w, in_sem.at[9]).wait()

    def project(r0, n):
        rows = slice(r0, r0 + n)
        for j in range(NT):
            cols = slice(j * 128, (j + 1) * 128)
            v = lat[rows, cols].astype(F32) * inv[rows, :] * mrow(0, j) + mrow(2, j)
            hbuf[rows, cols] = v.astype(BF16)
        o = jnp.dot(hbuf[rows, :], w[...], preferred_element_type=F32).astype(BF16)
        qb[rows, :] = o[:, 0:128]
        kv[0, OWN + r0 : OWN + r0 + n, :] = o[:, 128:256]
        kv[1, OWN + r0 : OWN + r0 + n, :] = o[:, 256:384]

    phase("own_kv")
    for i in range(2):
        pl.semaphore_wait(far_sem.at[i], 1)

    def ctx_rows(ref, n, at):
        sq = jnp.zeros((n, 128), F32)
        for j in range(NT):
            v = ref[0 : n // CR, :, j * 128 : (j + 1) * 128].astype(F32).reshape(n, 128)
            sq += v * v
        cinv = lax.rsqrt(jnp.sum(sq, axis=1, keepdims=True) * (1.0 / D) + EPS)
        cinv = jnp.broadcast_to(cinv, (n, 128))
        for j in range(NT):
            cols = slice(j * 128, (j + 1) * 128)
            v = ref[0 : n // CR, :, cols].astype(F32).reshape(n, 128)
            hbuf[at : at + n, cols] = (v * cinv * mrow(1, j) + mrow(3, j)).astype(BF16)

    v_copies = [
        rcopy(
            kown, farin.at[FAR.index(ZN - d)], v_sem.at[0], v_sem.at[1], sp_z(d), t,
        )
        for d in far_order
    ]

    @pl.when(odd)
    def _():
        at = TOK + NB
        hbuf[at : at + 16, :] = jnp.zeros((16, D), BF16)
        ctx_rows(craw, CR, at)
        o = jnp.dot(hbuf[at : at + 16, :], w[:, 128:384], preferred_element_type=F32)
        for i in range(2):
            kown[i] = o[0:CR, i * 128 : (i + 1) * 128].astype(BF16)
        for cp in v_copies:
            cp.start()

    phase("proj_edge")
    project(TOK - BEFORE * GW, BEFORE * GW)
    to_next = rcopy(
        kv.at[:, KVN - (BEFORE + AFTER) * GW : KVN - AFTER * GW, :], kv.at[:, 0:OWN, :],
        h_sem.at[0], h_sem.at[1], s + 1, t,
    )

    @pl.when(has_next)
    def _():
        to_next.start()

    phase("fwd")
    fy_copies = [
        rcopy(yraw.at[i, :, half], yraw.at[i, :, half], fs_sem.at[i], fr_sem.at[i], s, tp_of(0, 1))
        for i in range(YH)
    ]
    f_copy = rcopy(
        craw.at[1:, :, half], craw.at[1:, :, half], f_sem.at[0], f_sem.at[1], s, tp_of(0, 1)
    )
    for i in range(YH):

        @pl.when(y != 2 * i)
        def _():
            arrived(yraw.at[i, :, half], ur_sem, i).wait_recv()
            fy_copies[i].start()

    @pl.when(odd)
    def _():
        z_all.wait_recv()
        f_copy.start()

    phase("proj_first")
    project(0, BEFORE * GW)
    to_prev = rcopy(
        kv.at[:, OWN : OWN + AFTER * GW, :], kv.at[:, KVN - AFTER * GW : KVN, :],
        h_sem.at[2], h_sem.at[3], s - 1, t,
    )

    @pl.when(has_prev)
    def _():
        to_prev.start()

    phase("ctx_z")
    @pl.when(even)
    def _():
        own_row.wait()

    for i in range(YH):

        @pl.when(y != 2 * i)
        def _():
            fy_copies[i].wait_recv()

    at = TOK + NB + 16
    ctx_rows(yraw, ZB, at)
    o = jnp.dot(hbuf[at : at + ZB, :], w[:, 128:384], preferred_element_type=F32)
    for i in range(2):
        kvz[0, i] = o[:, i * 128 : (i + 1) * 128].astype(BF16)
    k_copies = [
        rcopy(kvz.at[0], kvz.at[ZN - d], k_sem.at[0], k_sem.at[1], sp_z(d), t)
        for d in by_hops(range(1, ZN))
    ]
    for cp in k_copies:
        cp.start()

    phase("ctx_kv")
    y_copies = [
        rcopy(kvn.at[yi], kvn.at[yi], y_sem.at[0], yr_sem.at[yi], sp_y(d), t) for d in y_order
    ]
    w_copies = [
        rcopy(kvf.at[yi], kvf.at[yi], y_sem.at[1], wr_sem.at[yi], sp_y(d), t) for d in y_order
    ]

    @pl.when(odd)
    def _():
        f_copy.wait_recv()
        ctx_rows(craw, NB, TOK)
        o = jnp.dot(hbuf[TOK : TOK + NB, :], w[:, 128:384], preferred_element_type=F32)
        for i in range(2):
            kvn[yi, i] = o[:, i * 128 : (i + 1) * 128].astype(BF16)
        for cp in y_copies:
            cp.start()

    phase("proj_mid")
    project(BEFORE * GW, TOK - 2 * BEFORE * GW)

    factor = HD ** (-0.5)
    base = s * ROWS

    def window(r):
        g = base + r
        first_row = jnp.clip(g - WR // 2, 0, ALL_ROWS - WR)
        a0 = first_row - g + WR - 1
        k0 = pl.multiple_of((first_row - base + BEFORE) * GW, GW)
        rows = slice(r * GW, (r + 1) * GW)
        keys = kv[0, pl.ds(k0, WR * GW), :]
        vals = kv[1, pl.ds(k0, WR * GW), :]
        sc = lax.dot_general(qb[rows, :], keys, NT_DIMS, preferred_element_type=F32) * factor
        sc = jnp.concatenate(
            [sc[:, i * 128 : (i + 1) * 128] + bias[a0 + 2 * i] for i in range(WR // 2)], axis=1
        )
        m = jnp.max(sc, axis=1, keepdims=True)
        p = jnp.exp(sc - m)
        mwin[rows, :] = jnp.broadcast_to(m, (GW, 128))
        lwin[rows, :] = jnp.broadcast_to(jnp.sum(p, axis=1, keepdims=True), (GW, 128))
        owin[rows, :] = jnp.dot(p.astype(BF16), vals, preferred_element_type=F32)

    phase("win_mid")
    for r in range(BEFORE, ROWS - AFTER):
        window(r)

    phase("await_far")

    @pl.when(odd)
    def _():
        v_all.wait_recv()
        for i in range(2):
            kvf[yi, i] = farin[:, i].astype(F32).reshape(FB, HD).astype(BF16)
        for cp in w_copies:
            cp.start()

    phase("await_halo")

    @pl.when(has_prev)
    def _():
        to_next.wait_recv()

    @pl.when(has_next)
    def _():
        to_prev.wait_recv()

    phase("win_edge")
    for r in (*range(BEFORE), *range(ROWS - AFTER, ROWS)):
        window(r)

    def merge(rows, parts):
        q = qb[rows, :]
        scs = []
        for ctx in parts:
            keys = ctx[:, 0].reshape(-1, HD)
            sc = lax.dot_general(q, keys, NT_DIMS, preferred_element_type=F32) * factor
            scs.append(sc)
        m0 = mwin[rows, :]
        tiles = [
            [sc[:, i * 128 : (i + 1) * 128] for i in range(sc.shape[1] // 128)] for sc in scs
        ]
        top = functools.reduce(jnp.maximum, sum(tiles, []))
        m = jnp.maximum(jnp.max(top, axis=1, keepdims=True), m0)
        alpha = jnp.exp(m0 - m)
        exps = [[jnp.exp(tile - m) for tile in part] for part in tiles]
        total = functools.reduce(jnp.add, sum(exps, []))
        den = alpha * lwin[rows, :] + jnp.sum(total, axis=1, keepdims=True)
        o = alpha * owin[rows, :]
        for ctx, part in zip(parts, exps):
            vals = ctx[:, 1].reshape(-1, HD)
            p = jnp.concatenate(part, axis=1).astype(BF16)
            o += jnp.dot(p, vals, preferred_element_type=F32)
        return m, den, o

    phase("await_y")
    for i in range(YH):

        @pl.when(y != 2 * i + 1)
        def _():
            arrived(kvn.at[i], yr_sem, i).wait_recv()

    phase("ctx_near")
    for b in range(4):
        rows = slice(b * 160, (b + 1) * 160)
        mwin[rows, :], lwin[rows, :], owin[rows, :] = merge(rows, (kvn.at[0:YH],))
    phase("await_k")
    for i in range(YH):

        @pl.when(y != 2 * i + 1)
        def _():
            arrived(kvf.at[i], wr_sem, i).wait_recv()

    phase("await_k2")
    k_all.wait_recv()
    phase("ctx_attn")
    for pair in ((2, 1), (3,), (0,)):
        done = []
        for dx in pair:
            chip = lax.rem(x + dx, XN)
            _, den, o = merge(pl.ds(pl.multiple_of(chip * 160, 160), 160), (kvf.at[0:YH], kvz))
            done.append((o / den).astype(BF16))
        for dx, o in zip(pair, done):
            attn[2 * dx] = o[0:80]
            attn[2 * dx + 1] = o[80:160]
        for dx in pair:
            chip = lax.rem(x + dx, XN)
            if dx == 0:
                rcopy(attn.at[1 - c], own.at[c], o_sem.at[0], or_sem.at[0], s, tp_of(0, 1)).start()
                own[c] = attn[c]
                continue
            for cc in range(2):
                rcopy(
                    attn.at[2 * dx + cc], own.at[2 * dx + c], o_sem.at[0], or_sem.at[dx],
                    s, chip * 2 + cc,
                ).start()

    phase("out_proj")
    with jax.named_scope("await_g"):
        g_all.wait_recv()
    for f in range(2):
        hh = c if f == 0 else 1 - c
        mod[hh, 4] = redg[f] + redg[2 + f] + redg[4 + f] + redg[6 + f]
    loads["ow"].wait()
    for n, dx in enumerate((0, 1, 3, 2)):
        got = own.at[1 - c] if dx == 0 else own.at[2 * dx : 2 * dx + 2]
        rcopy(got, got, o_sem.at[0], or_sem.at[dx], s, tp_of(0, 1)).wait_recv()
        lhs = jnp.concatenate([own[2 * dx], own[2 * dx + 1]], axis=1)
        chip = lax.rem(x + XN - dx, XN)
        wrows = pl.ds(pl.multiple_of(chip * 256, 256), 256)
        res = pl.ds(pl.multiple_of(t * 80, 80), 80)
        for q in range(8):
            cols = slice(q * 256, (q + 1) * 256)
            o = jnp.dot(lhs, wo[wrows, cols], preferred_element_type=F32)
            if n > 0:
                o += acc[:, cols]
            if n < 3:
                acc[:, cols] = o
            else:
                for i in range(2):
                    j = 2 * q + i
                    jc = slice(j * 128, (j + 1) * 128)
                    v = lat[res, jc].astype(F32) + mrow(4, j) * o[:, i * 128 : (i + 1) * 128]
                    out_ref[:, jc] = v.astype(BF16)

    phase("drain")
    for cp in (a_copy, g_copy, b_all, g_all, k_all, o_all):
        cp.wait_send()

    @pl.when(odd)
    def _():
        for cp in (f_copy, z_all, v_all, y_all, w_all):
            cp.wait_send()

    @pl.when(even)
    def _():
        u_all.wait_send()

    for i in range(YH):

        @pl.when(y != 2 * i)
        def _():
            fy_copies[i].wait_send()

    @pl.when(has_next)
    def _():
        to_next.wait_send()

    @pl.when(has_prev)
    def _():
        to_prev.wait_send()

    phase(None)


def shards(
    latents, cond, ctx_cond, context, norm_gain, shift_weight, scale_weight, gate_weight,
    q_weight, k_weight, v_weight, out_weight, rel_bias,
):
    dma = pltpu.SemaphoreType.DMA
    scratch = [
        pltpu.VMEM((TOK, D), BF16),
        pltpu.VMEM((2, NT, 128), F32),
        pltpu.VMEM((len(NEAR), CR, D), BF16),
        pltpu.VMEM((NT, 128), F32),
        pltpu.VMEM((3, 256, D), BF16),
        pltpu.VMEM((D, 384), BF16),
        pltpu.VMEM((1024, D), BF16),
        pltpu.VMEM((15, 1, 31), F32),
        pltpu.VMEM((2, 5, 8, 128), F32),
        pltpu.VMEM((5, 8, 128), F32),
        pltpu.VMEM((2 * XN, 4, 8, 128), BF16),
        pltpu.VMEM((2 * XN, 8, 128), F32),
        pltpu.VMEM((2, 5, 8, 128), F32),
        pltpu.VMEM((TOK, 128), F32),
        pltpu.VMEM((14, GW, 128), F32),
        pltpu.VMEM((TOK + NB + 16 + ZB, D), BF16),
        pltpu.VMEM((TOK, HD), BF16),
        pltpu.VMEM((2, KVN, HD), BF16),
        pltpu.VMEM((2, CR, HD), BF16),
        pltpu.VMEM((len(FAR), 2, CR, HD), BF16),
        pltpu.VMEM((YN, 2, NB, HD), BF16),
        pltpu.VMEM((YN, 2, FB, HD), BF16),
        pltpu.VMEM((ZN, 2, ZB, HD), BF16),
        pltpu.VMEM((YH, CR, D), BF16),
        pltpu.VMEM((TOK, HD), F32),
        pltpu.VMEM((TOK, HD), F32),
        pltpu.VMEM((TOK, HD), F32),
        pltpu.VMEM((8, 80, HD), BF16),
        pltpu.VMEM((8, 80, HD), BF16),
        pltpu.VMEM((80, D), F32),
        dma((11,)), dma((4,)), dma((4,)), dma((2,)), dma((2,)), dma((2,)), dma((YH,)),
        dma((YH,)), dma((2,)), pltpu.SemaphoreType.REGULAR((2,)), dma((2,)), dma((YH,)), dma((YH,)),
        dma((YH,)), dma((2,)), dma((4,)), dma((2,)), dma((XN,)),
    ]
    anyspec = pl.BlockSpec(memory_space=pl.ANY)
    operands = (
        latents, cond.reshape(NT, 128), ctx_cond.reshape(NT, 128), context, norm_gain.reshape(NT, 128),
        shift_weight, scale_weight, gate_weight, q_weight, k_weight, v_weight, out_weight,
        rel_bias.transpose(1, 0, 2),
    )
    return pl.pallas_call(
        body,
        out_shape=jax.ShapeDtypeStruct((80, D), BF16),
        in_specs=[anyspec] * len(operands),
        out_specs=pl.BlockSpec(memory_space=pltpu.VMEM),
        scratch_shapes=scratch,
        compiler_params=pltpu.CompilerParams(
            collective_id=0, has_side_effects=True, vmem_limit_bytes=40 * 1024 * 1024
        ),
        name="step",
    )(*(pltpu.with_memory_space_constraint(v, pltpu.HBM) for v in operands))


def solution(mesh):
    in_specs = (
        P("sp", None),
        P(),
        P(),
        P("sp", None),
        P(),
        P("tp", None),
        P("tp", None),
        P("tp", None),
        P(None, "tp"),
        P(None, "tp"),
        P(None, "tp"),
        P(),
        P("tp", None, None),
    )
    out_specs = P(("sp", "tp"), None)
    return jax.shard_map(shards, mesh=mesh, in_specs=in_specs, out_specs=out_specs, check_vma=False)
```
